256 devices in a mesh: vp: 16 (over y, x), dp: 16 (over z, core).
Axes of the slice: x: 4, y: 4, z: 8, core: 2. Of those that a mesh axis runs over, the one named last changes fastest.
Arguments:
- hidden_act: bfloat16 [8192, 8192], P('dp', 'vp'), may hold values from 0 to 36
- down_weight: bfloat16 [8192, 2048], P('vp'), may hold values from -0.0625 to 0.0625
- residual: bfloat16 [8192, 2048], P(('dp', 'vp')), may hold values from -300 to 300
- post_gain: float32 [2048], replicated, may hold values from 0.1 to 1.9
- final_gain: float32 [2048], replicated, may hold values from 0.1 to 1.9
- vocab: bfloat16 [2048, 32768], P(None, 'vp'), may hold values from -0.33 to 0.33
- vocab_bias: float32 [32768], P('vp'), may hold values from -2.5 to 2.5
- target_ids: int32 [8192, 4], P('dp'), may hold values from 0 to 32767
- target_weights: float32 [8192, 4], P('dp'), may hold values from 0 to 1, as said below
Outputs:
- losses: float32 [8192], P(('dp', 'vp'))
- stream_grad: float32 [8192, 2048], P(('dp', 'vp'))
- vocab_grad: float32 [2048, 32768], P('dp', 'vp')
The draws below stay inside these ranges and needn't reach their ends.
Inputs may be any that keep to these rules, and one draw needn't show every extreme that they name: `target_weights`: the 4 weights of a token add up to one.
All inputs are finite; a program needn't handle non-finite values.
Results may differ from the reference program's by a relative error of at most 0.01225.
Values may be sent and summed in bfloat16 or wider, within the bound.
A program may use at most 128 MiB of HBM per device.

```python
import math
import jax
import jax.numpy as jnp
import numpy as np
from jax import lax

D = 2048
FF = 8192
V = 32768
TOPK = 4
TOK_GRP = 512
TOKENS = 8192
N_VP = 16
N_DP = 16


def spike_signs(key):
    return (jax.random.randint(jax.random.fold_in(key, 4242), (D,), 0, 2) * 2 - 1).astype(jnp.float32)


def draw_hidden_act(key, part):
    values = jax.random.normal(jax.random.fold_in(key, 41), (TOKENS, FF), jnp.float32)
    values = jnp.clip(values, -6.0, 6.0)
    positive = jnp.maximum(values, 0.0)
    return (positive * positive).astype(jnp.bfloat16)


def draw_residual(key, part):
    values = jnp.clip(jax.random.normal(jax.random.fold_in(key, 11), (TOKENS, D), jnp.float32), -6.0, 6.0)
    marked = (jnp.arange(TOKENS) % 61 == 3)[:, None]
    values = jnp.where(marked, 300.0 * spike_signs(key)[None, :], values)
    return values.astype(jnp.bfloat16)


def draw_vocab(key, part):
    values = 0.055 * jnp.clip(jax.random.normal(jax.random.fold_in(key, 21), (D, V), jnp.float32), -6.0, 6.0)
    marked = (jnp.arange(V) % 509 == 7)[None, :]
    values = jnp.where(marked, 256.0 / D * spike_signs(key)[:, None], values)
    return values.astype(jnp.bfloat16)


def draw_vocab_bias(key, part):
    offsets = jax.random.uniform(jax.random.fold_in(key, 31), (N_VP,), jnp.float32, -1.5, 1.5)
    shard_of = jnp.arange(V) // (V // N_VP)
    values = 0.5 * jnp.clip(jax.random.normal(jax.random.fold_in(key, 32), (V,), jnp.float32), -2.0, 2.0)
    return offsets[shard_of] + values


def draw_target_weights(key, part):
    logits = 1.5 * jax.random.normal(jax.random.fold_in(key, 52), (TOKENS, TOPK), jnp.float32)
    return jax.nn.softmax(logits, axis=-1)


def place_ends(entries, key, smallest, top_value):
    spot = [jax.random.randint(jax.random.fold_in(key, axis), (), 0, length) for axis, length in enumerate(entries.shape)]
    widest = entries.shape.index(max(entries.shape))
    next_to = spot[:widest] + [(spot[widest] + 1) % entries.shape[widest]] + spot[widest + 1:]
    return entries.at[tuple(spot)].set(smallest).at[tuple(next_to)].set(top_value)


def steps_of(own_key, extent, cuts, low, largest):
    factor_of = 1.0
    for axis_at, parts in cuts:
        draws = jax.random.uniform(jax.random.fold_in(jax.random.fold_in(own_key, 6), axis_at), (parts,), jnp.float32, low / len(cuts), largest / len(cuts))
        factor_of = factor_of * jnp.repeat(jnp.exp(draws), extent[axis_at] // parts).reshape((-1,) + (1,) * (len(extent) - 1 - axis_at))
    return factor_of


def rank_table(amount, slope):
    weights = [(1 << 20) // math.isqrt(standing ** slope) + 1 for standing in range(1, amount + 1)]
    scale = 1 + sum(weights) // (1 << 30)
    return np.cumsum(np.array([max(1, weight // scale) for weight in weights]))


def ranked_ids(stream_key, shape, count, slope):
    table = rank_table(count, slope)
    pick = jax.random.randint(jax.random.fold_in(stream_key, 1), shape, 0, int(table[count - 1]))
    standing = jnp.searchsorted(jnp.asarray(table, jnp.int32), pick, side="right")
    return jax.random.permutation(jax.random.fold_in(stream_key, 2), count)[standing].astype(jnp.int32)


def centred(key, dims, scale, reach, pieces=(), kind=jnp.bfloat16):
    values = scale * jax.random.normal(key, dims, jnp.float32)
    if pieces:
        values = values * steps_of(key, dims, pieces, -0.22, 0.18)
    return jnp.clip(values, -reach, reach).astype(kind)


def setup_inputs(seed: int = 0) -> dict:
    splits = jax.random.split(jax.random.key(seed), 10)
    hidden_act = draw_hidden_act(jax.random.fold_in(splits[9], 71), 0)
    down_weight = centred(splits[1], (FF, D), FF ** -0.5, 0.0625, ((0, 16),))
    residual = draw_residual(jax.random.fold_in(splits[9], 71), 0)
    post_gain = jnp.clip(1.0 + 0.18 * jax.random.normal(splits[3], (D,), jnp.float32), 0.1, 1.9)
    final_gain = jnp.clip(1.0 + 0.18 * jax.random.normal(splits[4], (D,), jnp.float32), 0.1, 1.9)
    vocab = draw_vocab(jax.random.fold_in(splits[9], 71), 0)
    vocab_bias = draw_vocab_bias(jax.random.fold_in(splits[9], 71), 0)
    target_ids = place_ends(ranked_ids(splits[7], (TOKENS, TOPK), V, 2), jax.random.fold_in(splits[7], 3), 0, V - 1).astype(jnp.int32)
    target_weights = draw_target_weights(jax.random.fold_in(splits[9], 71), 0)
    return dict(hidden_act=hidden_act, down_weight=down_weight, residual=residual, post_gain=post_gain, final_gain=final_gain, vocab=vocab, vocab_bias=vocab_bias, target_ids=target_ids, target_weights=target_weights)


epsilon = 1e-06
z_weight = 0.001
loss_scale = 32.0

def inverse_rms(values):
    return lax.rsqrt(lax.optimization_barrier(jnp.mean(values * values, axis=-1, keepdims=True)) + epsilon)

def reference(hidden_act, down_weight, residual, post_gain, final_gain, vocab, vocab_bias, target_ids, target_weights):
    branch = jnp.dot(hidden_act, down_weight, preferred_element_type=jnp.float32)
    stream = residual.astype(jnp.float32) + branch * inverse_rms(branch) * post_gain
    inverse = inverse_rms(stream)
    normed = (stream * inverse * final_gain).astype(jnp.bfloat16)
    columns = jnp.arange(V, dtype=jnp.int32)[None, :]

    def group(matrix_acc, inputs):
        row_block, target_block, weight_block = inputs
        scores = jnp.dot(row_block, vocab, preferred_element_type=jnp.float32) + vocab_bias
        row_max = lax.optimization_barrier(jnp.max(scores, axis=1))
        row_sum = lax.optimization_barrier(jnp.sum(jnp.exp(scores - row_max[:, None]), axis=1))
        log_norm = row_max + jnp.log(row_sum)
        wanted = jnp.zeros(scores.shape, jnp.float32)
        for target_k in range(TOPK):
            wanted = wanted + jnp.where(target_block[:, target_k:target_k + 1] == columns, weight_block[:, target_k:target_k + 1], 0.0)
        target_score = lax.optimization_barrier(jnp.sum(wanted * scores, axis=1))
        losses = log_norm - target_score + z_weight * log_norm * log_norm
        probability = jnp.exp(scores - log_norm[:, None])
        score_grads = (loss_scale * (probability * (1.0 + 2.0 * z_weight * log_norm)[:, None] - wanted)).astype(jnp.bfloat16)
        row_grad = lax.dot_general(score_grads, vocab, (((1,), (1,)), ((), ())), preferred_element_type=jnp.float32)
        matrix_acc = matrix_acc + lax.dot_general(row_block, score_grads, (((0,), (0,)), ((), ())), preferred_element_type=jnp.float32)
        return (matrix_acc, (losses, row_grad))
    stacked = (normed.reshape(N_DP, TOK_GRP, D), target_ids.reshape(N_DP, TOK_GRP, TOPK), target_weights.reshape(N_DP, TOK_GRP, TOPK))
    vocab_grad, outputs = lax.scan(group, jnp.zeros((D, V), jnp.float32), stacked)
    losses = outputs[0].reshape(TOKENS)
    row_grad = outputs[1].reshape(TOKENS, D)
    upstream = row_grad * final_gain
    stream_grad = inverse * (upstream - stream * inverse * inverse * lax.optimization_barrier(jnp.mean(upstream * stream, axis=-1, keepdims=True)))
    return (losses, stream_grad, vocab_grad)
```

```python
import jax
import jax.numpy as jnp
from jax import lax
from jax.experimental import pallas as pl
from jax.experimental.pallas import tpu as pltpu
from jax.sharding import Mesh
from jax.sharding import PartitionSpec as P

MESH = pl.DeviceIdType.MESH
F32 = jnp.float32
BF16 = jnp.bfloat16
AXES = ("y", "x", "z", "c")

EPSILON = 1e-06
Z_WEIGHT = 0.001
LOSS_SCALE = 32.0

RING = 4
NZ = 8
BLOCK = 32
HALF = 16
CHUNK = 128
ROWS = 512
WIDTH = 2048
COLS = 2048
SUB = 512
NSUB = COLS // SUB
RS_ORDER = (2, 1, 3, 0)
AG_ORDER = (0, 3, 1, 2)


def inverse_rms(values):
    return lax.rsqrt(jnp.mean(values * values, axis=-1, keepdims=True) + EPSILON)


def aligned(start, size, unit):
    return pl.ds(pl.multiple_of(start, unit), size)


def kernel(
    hid, down, res, pg, fg, voc, bias, ids, wts,
    loss_o, sg_o, vg_o,
    hid_v, down_v, res_v, pg_v, fg_v, voc_v, bias_v, ids_v, wts_v,
    part, scores, wanted, normed, grads, stream_v, inv_v,
    ra, rb, rc, sb2, ra2, rb2, rc2, keep2,
    rra, rrb, rrc, rsb2, rra2, rrb2, rrc2,
    lse_c, tgt_c, norm_c, stat_s, stat_r, loss_v,
    v_own, pair_s, pair_r, z_s, z_r, sg_v, vg_v,
    load_sem, hid_sem, out_sem,
    rs_ss, rs_rs, rr_ss, rr_rs, ag_ss, ag_rs, st_ss, st_rs, pr_ss, pr_rs, z_ss, z_rs,
):
    y, x, z, c = (lax.axis_index(name) for name in AXES)
    a = x + c * (y - x)
    b = y + c * (x - y)

    def mod4(value):
        return lax.rem(value, RING)

    def dev_a(step):
        to = mod4(a + step)
        return (y + c * (to - y), to + c * (x - to), z, c)

    def dev_b(step):
        to = mod4(b + step)
        return (to + c * (y - to), x + c * (to - x), z, c)

    up_z = lax.rem(z + 1 + c * (NZ - 2), NZ)
    down_z = lax.rem(z + NZ - 1 - c * (NZ - 2), NZ)
    dev_up = (y, x, up_z, c)
    dev_down = (y, x, down_z, c)
    dev_pair = (y, x, z, 1 - c)

    def source_row(i, q):
        return (i * (1 + 3 * c) + q * (4 - 3 * c)) * BLOCK

    def rows(i, q, h):
        return aligned(i * CHUNK + q * BLOCK + h * HALF, HALF, HALF)

    def rows32(i, q):
        return aligned(i * CHUNK + q * BLOCK, BLOCK, BLOCK)

    def chunk_rows(i):
        return aligned(i * CHUNK, CHUNK, CHUNK)

    def sub_cols(j):
        return aligned(j * SUB, SUB, SUB)

    def remote(src, dst, send, recv, to):
        return pltpu.make_async_remote_copy(
            src_ref=src, dst_ref=dst, send_sem=send, recv_sem=recv,
            device_id=to, device_id_type=MESH,
        )

    a_up, a_dn, a_far = dev_a(1), dev_a(3), dev_a(2)
    b_up, b_dn, b_far = dev_b(1), dev_b(3), dev_b(2)

    barrier = pltpu.get_barrier_semaphore()
    for to in (a_up, a_dn, a_far, b_up, b_dn, b_far, dev_pair, dev_down):
        pl.semaphore_signal(barrier, inc=1, device_id=to, device_id_type=MESH)

    hid_copies = []
    for i in range(RING):
        for q in range(RING):
            hid_copies.append(
                pltpu.make_async_copy(
                    hid.at[aligned(source_row(i, q), BLOCK, BLOCK), :],
                    hid_v.at[pl.ds(i * CHUNK + q * BLOCK, BLOCK), :],
                    hid_sem.at[i * RING + q],
                )
            )
    loads = [
        pltpu.make_async_copy(src, dst, load_sem.at[k])
        for k, (src, dst) in enumerate(
            [
                (down, down_v), (ids, ids_v), (wts, wts_v), (res, res_v),
                (pg, pg_v), (fg, fg_v), (bias, bias_v),
            ]
            + [
                (voc.at[pl.ds(k * SUB, SUB), :], voc_v.at[pl.ds(k * SUB, SUB), :])
                for k in range(WIDTH // SUB)
            ]
        )
    ]
    for copy in hid_copies + loads:
        copy.start()

    def branch_chunk(i, send):
        def piece(n, carry):
            value = jnp.dot(
                hid_v[chunk_rows(i), :], down_v[:, sub_cols(n)], preferred_element_type=F32
            )
            scores[chunk_rows(i), sub_cols(n)] = value
            if send:
                part[chunk_rows(i), sub_cols(n)] = value.astype(BF16)
            return carry

        lax.fori_loop(0, WIDTH // SUB, piece, 0)

    def rs_tools(ra, rb, rc, sb2, ra2, rb2, rc2, ss, rs):
        far, up, dn = mod4(a + 2), mod4(a + 1), mod4(a + 3)

        def q_of(t):
            return mod4(b + RS_ORDER[t])

        def one(kind, t):
            q, k = q_of(t), kind * RING + t
            src, dst, to = (
                (rows(far, q, 0), ra.at[0, t], a_up),
                (rows(far, q, 1), ra.at[1, t], a_dn),
                (rows(up, q, 1), rb.at[0, t], a_up),
                (rows(dn, q, 0), rb.at[1, t], a_dn),
                (rows(up, q, 0), rc.at[0, t], a_up),
                (rows(dn, q, 1), rc.at[1, t], a_dn),
            )[kind]
            return remote(part.at[src, :], dst, ss.at[k], rs.at[k], to)

        def two(kind):
            k = 24 + kind
            src, dst, to = (
                (sb2.at[0, 0], ra2.at[0], b_up),
                (sb2.at[0, 1], ra2.at[1], b_dn),
                (sb2.at[1, 1], rb2.at[0], b_up),
                (sb2.at[2, 0], rb2.at[1], b_dn),
                (sb2.at[1, 0], rc2.at[0], b_up),
                (sb2.at[2, 1], rc2.at[1], b_dn),
            )[kind]
            return remote(src, dst, ss.at[k], rs.at[k], to)

        def first():
            for t in range(RING):
                one(0, t).start()
                one(1, t).start()

        def middle():
            for t in range(RING):
                q = q_of(t)
                one(2, t).start()
                one(3, t).start()
                for kind, i, h in ((0, up, 0), (1, dn, 1)):
                    one(kind, t).wait_recv()
                    part[rows(i, q, h), :] = (
                        scores[rows(i, q, h), :] + ra[h, t].astype(F32)
                    ).astype(BF16)
                    one(4 + kind, t).start()

        def finish_a():
            for t in range(RING):
                q = q_of(t)
                for kind in range(2, 6):
                    one(kind, t).wait_recv()
                low = scores[rows(a, q, 0), :] + rc[0, t].astype(F32) + rb[1, t].astype(F32)
                high = scores[rows(a, q, 1), :] + rb[0, t].astype(F32) + rc[1, t].astype(F32)
                if t == 0:
                    sb2[0, 0] = low.astype(BF16)
                    two(0).start()
                    sb2[0, 1] = high.astype(BF16)
                    two(1).start()
                elif t == 1:
                    sb2[1, 1] = high.astype(BF16)
                    two(2).start()
                    keep2[0] = low
                elif t == 2:
                    sb2[2, 0] = low.astype(BF16)
                    two(3).start()
                    keep2[1] = high
                else:
                    keep2[2] = low
                    keep2[3] = high

        def middle_b():
            two(0).wait_recv()
            sb2[1, 0] = (keep2[0] + ra2[0].astype(F32)).astype(BF16)
            two(4).start()
            two(1).wait_recv()
            sb2[2, 1] = (keep2[1] + ra2[1].astype(F32)).astype(BF16)
            two(5).start()

        def finish_b():
            for kind in range(2, 6):
                two(kind).wait_recv()
            low = keep2[2] + rc2[0].astype(F32) + rb2[1].astype(F32)
            high = keep2[3] + rb2[0].astype(F32) + rc2[1].astype(F32)
            return jnp.concatenate([low, high], axis=0)

        def sent():
            for kind in range(6):
                for t in range(RING):
                    one(kind, t).wait_send()
            for kind in range(6):
                two(kind).wait_send()

        return first, middle, finish_a, middle_b, finish_b, sent

    def wanted_block(p):
        i, q = p // RING, lax.rem(p, RING)
        at = aligned(source_row(i, q), BLOCK, BLOCK)
        local = ids_v[at, :] - (y * RING + x) * COLS
        weight = wts_v[at, :]
        for n in range(NSUB):
            position = lax.broadcasted_iota(jnp.int32, (BLOCK, SUB), 1) + n * SUB
            total = jnp.zeros((BLOCK, SUB), F32)
            for k in range(4):
                total = total + jnp.where(
                    local[:, k : k + 1] == position, weight[:, k : k + 1], 0.0
                )
            wanted[aligned(p * BLOCK, BLOCK, BLOCK), pl.ds(n * SUB, SUB)] = total

    def wanted_blocks(start, stop):
        def body(p, carry):
            wanted_block(p)
            return carry

        lax.fori_loop(start, stop, body, 0)

    first, middle, finish_a, middle_b, finish_b, sent = rs_tools(
        ra, rb, rc, sb2, ra2, rb2, rc2, rs_ss, rs_rs
    )
    for copy in hid_copies:
        copy.wait()
    loads[0].wait()
    branch_chunk(mod4(a + 2), True)
    pl.semaphore_wait(barrier, 8)
    first()
    branch_chunk(mod4(a + 1), True)
    branch_chunk(mod4(a + 3), True)
    branch_chunk(a, False)
    for copy in loads[1:7]:
        copy.wait()
    wanted_blocks(0, 8)
    middle()
    wanted_blocks(8, 16)
    finish_a()
    middle_b()
    branch = finish_b()

    stream = res_v[...].astype(F32) + branch * inverse_rms(branch) * pg_v[...]
    inverse = inverse_rms(stream)
    stream_v[...] = stream
    inv_v[...] = jnp.broadcast_to(inverse, inv_v.shape)
    normed[rows32(a, b), :] = (stream * inverse * fg_v[...]).astype(BF16)

    up, dn, far = mod4(a + 1), mod4(a + 3), mod4(a + 2)
    b1, b3, b2 = mod4(b + 1), mod4(b + 3), mod4(b + 2)

    def gather_b(kind, arriving=False):
        at, to = (
            (rows32(a, b3 if arriving else b), b_up),
            (rows32(a, b1 if arriving else b), b_dn),
            (rows(a, b2 if arriving else b3, 0), b_up),
            (rows(a, b2 if arriving else b1, 1), b_dn),
        )[kind]
        return remote(normed.at[at, :], normed.at[at, :], ag_ss.at[kind], ag_rs.at[kind], to)

    def gather_a(kind, t, arriving=False):
        q = mod4(b + AG_ORDER[t])
        at, to = (
            (rows32(dn if arriving else a, q), a_up),
            (rows32(up if arriving else a, q), a_dn),
            (rows(far if arriving else dn, q, 0), a_up),
            (rows(far if arriving else up, q, 1), a_dn),
        )[kind]
        k = 4 + t * 4 + kind
        return remote(normed.at[at, :], normed.at[at, :], ag_ss.at[k], ag_rs.at[k], to)

    def forward_a(t):
        for kind in (0, 1):
            gather_a(kind, t, True).wait_recv()
            gather_a(2 + kind, t).start()

    for kind in (0, 1):
        gather_b(kind).start()
        gather_a(kind, 0).start()
    for kind in (0, 1):
        gather_b(kind, True).wait_recv()
        gather_b(2 + kind).start()
        gather_a(0, 1 + kind).start()
        gather_a(1, 1 + kind).start()
    forward_a(0)
    for kind in (2, 3):
        gather_b(kind, True).wait_recv()
    for kind in (0, 1):
        gather_a(kind, 3).start()
    for copy in loads[7:]:
        copy.wait()

    def score_pieces(i, start, stop):
        def piece(n, carry):
            value = jnp.dot(
                normed[chunk_rows(i), :], voc_v[:, sub_cols(n)], preferred_element_type=F32
            )
            scores[chunk_rows(i), sub_cols(n)] = value + bias_v[:, sub_cols(n)]
            return carry

        lax.fori_loop(start, stop, piece, 0)

    def stats(i):
        def body(r, carry):
            at = aligned(i * CHUNK + r * HALF, HALF, HALF)
            value = scores[at, :]
            peak = jnp.max(value, axis=1, keepdims=True)
            total = jnp.sum(jnp.exp(value - peak), axis=1, keepdims=True)
            target = jnp.sum(wanted[at, :] * value, axis=1, keepdims=True)
            lse_c[at, :] = jnp.broadcast_to(peak + jnp.log(total), (HALF, 128))
            tgt_c[at, :] = jnp.broadcast_to(target, (HALF, 128))
            return carry

        lax.fori_loop(0, CHUNK // HALF, body, 0)
        stat_s[0, pl.ds(i, 1), :] = jnp.transpose(lse_c[chunk_rows(i), :])[0:1, :]
        stat_s[0, pl.ds(i + RING, 1), :] = jnp.transpose(tgt_c[chunk_rows(i), :])[0:1, :]

    score_pieces(a, 0, 2)
    forward_a(1)
    score_pieces(a, 2, 4)
    forward_a(2)
    stats(a)
    forward_a(3)
    for i in (up, dn):
        score_pieces(i, 0, 4)
        stats(i)
    for t in range(RING):
        for kind in (2, 3):
            gather_a(kind, t, True).wait_recv()
    score_pieces(far, 0, 4)
    stats(far)

    def stat_copy(phase, k):
        to = ((a_up, a_dn, a_far), (b_up, b_dn, b_far))[phase][k]
        n = phase * 3 + k
        return remote(stat_s.at[phase], stat_r.at[n], st_ss.at[n], st_rs.at[n], to)

    is_lse = lax.broadcasted_iota(jnp.int32, (8, 128), 0) < RING
    for phase in range(2):
        for k in range(3):
            stat_copy(phase, k).start()
        for k in range(3):
            stat_copy(phase, k).wait_recv()
        parts = [stat_s[phase]] + [stat_r[phase * 3 + k] for k in range(3)]
        peak = jnp.maximum(jnp.maximum(parts[0], parts[1]), jnp.maximum(parts[2], parts[3]))
        joint = peak + jnp.log(sum(jnp.exp(value - peak) for value in parts))
        stat_s[phase + 1] = jnp.where(is_lse, joint, sum(parts))
    log_rows = stat_s[2, 0:RING, :]
    for i in range(RING):
        norm_c[pl.ds(i * CHUNK, CHUNK), :] = jnp.transpose(
            jnp.broadcast_to(stat_s[2, i : i + 1, :], (CHUNK, 128))
        )
    loss_v[...] = log_rows - stat_s[2, RING:8, :] + Z_WEIGHT * log_rows * log_rows

    def grad_block(j):
        def body(r, carry):
            at = aligned(r * BLOCK, BLOCK, BLOCK)
            log_norm = norm_c[at, :]
            factor = 1.0 + 2.0 * Z_WEIGHT * log_norm
            for n in range(SUB // 128):
                cols = aligned(j * SUB + n * 128, 128, 128)
                probability = jnp.exp(scores[at, cols] - log_norm)
                grads[at, cols] = (
                    LOSS_SCALE * (probability * factor - wanted[at, cols])
                ).astype(BF16)
            return carry

        lax.fori_loop(0, ROWS // BLOCK, body, 0)

    def pair_copy(s, j):
        k = s * NSUB + j
        return remote(pair_s.at[k], pair_r.at[k], pr_ss.at[k], pr_rs.at[k], dev_pair)

    def z_copy(s, j):
        k = s * NSUB + j
        return remote(z_s.at[k], z_r.at[k], z_ss.at[k], z_rs.at[k], dev_up)

    def vocab_piece(s, j):
        away = (1 - 2 * c) * (1 + s)
        own_dest = lax.rem(z + 2 * NZ - away, NZ) * 2 + c
        pair_dest = lax.rem(z + 2 * NZ + away, NZ) * 2 + 1 - c
        both = jnp.concatenate(
            [normed[:, aligned(dest * CHUNK, CHUNK, CHUNK)] for dest in (own_dest, pair_dest)], axis=1
        )
        value = lax.dot_general(
            both, grads[:, sub_cols(j)], (((0,), (0,)), ((), ())), preferred_element_type=F32
        )
        v_own[(s % 2) * NSUB + j] = value[0:CHUNK]
        pair_s[s * NSUB + j] = value[CHUNK:].astype(BF16)
        pair_copy(s, j).start()

    def z_piece(s, j):
        k = s * NSUB + j
        pair_copy(s, j).wait_recv()
        value = v_own[(s % 2) * NSUB + j] + pair_r[k].astype(F32)
        if s > 0:
            z_copy(s - 1, j).wait_recv()
            value = value + z_r[k - NSUB].astype(F32)
        if s < NZ - 1:
            z_s[k] = value.astype(BF16)
            z_copy(s, j).start()
        else:
            vg_v[j] = value
            out_copy(j).start()

    def out_copy(j):
        return pltpu.make_async_copy(vg_v.at[j], vg_o.at[:, sub_cols(j)], out_sem.at[j])

    def row_piece(i, n):
        value = lax.dot_general(
            grads[chunk_rows(i), :], voc_v[sub_cols(n), :],
            (((1,), (1,)), ((), ())), preferred_element_type=F32,
        )
        scores[chunk_rows(i), sub_cols(n)] = value
        part[chunk_rows(i), sub_cols(n)] = value.astype(BF16)

    for j in range(NSUB):
        grad_block(j)
        vocab_piece(0, j)
        if j > 0:
            z_piece(0, j - 1)
    z_piece(0, NSUB - 1)
    sent()

    first, middle, finish_a, middle_b, finish_b, sent_rows = rs_tools(
        rra, rrb, rrc, rsb2, rra2, rrb2, rrc2, rr_ss, rr_rs
    )
    row_order = (far, up, dn, a)
    for s in range(NZ):

        def slot(j, carry):
            if s > 0:
                z_piece(s, j)
            if s < NZ - 1:
                vocab_piece(s + 1, j)
            if s < RING:
                row_piece(row_order[s], j)
            return carry

        lax.fori_loop(0, NSUB, slot, 0)
        if s == 0:
            first()
        elif s == 2:
            middle()
        elif s == 4:
            finish_a()
        elif s == 5:
            middle_b()
        elif s == 6:
            stream = stream_v[...]
            inverse = inv_v[:, 0:1]
            upstream = finish_b() * fg_v[...]
            sg_v[...] = inverse * (
                upstream
                - stream * inverse * inverse * jnp.mean(upstream * stream, axis=-1, keepdims=True)
            )
            pltpu.make_async_copy(sg_v, sg_o, out_sem.at[NSUB]).start()
            own = jnp.broadcast_to(loss_v[pl.ds(a, 1), :], (8, 128))
            own = pltpu.roll(own, lax.rem(128 - b * BLOCK, 128), 1)
            loss_o[...] = own[0:1, 0:BLOCK]

    sent_rows()
    for kind in range(4):
        gather_b(kind).wait_send()
        for t in range(RING):
            gather_a(kind, t).wait_send()
    for phase in range(2):
        for k in range(3):
            stat_copy(phase, k).wait_send()

    def drain_pair(k, carry):
        pair_copy(0, k).wait_send()
        return carry

    def drain_z(k, carry):
        z_copy(0, k).wait_send()
        return carry

    lax.fori_loop(0, NZ * NSUB, drain_pair, 0)
    lax.fori_loop(0, (NZ - 1) * NSUB, drain_z, 0)
    for j in range(NSUB):
        out_copy(j).wait()
    pltpu.make_async_copy(sg_v, sg_o, out_sem.at[NSUB]).wait()


def shards(hid, down, res, pg, fg, voc, bias, ids, wts):
    hbm = pl.BlockSpec(memory_space=pl.ANY)
    vmem = pltpu.VMEM
    dma = pltpu.SemaphoreType.DMA
    rs_bufs = [
        vmem((2, RING, HALF, WIDTH), BF16),
        vmem((2, RING, HALF, WIDTH), BF16),
        vmem((2, RING, HALF, WIDTH), BF16),
        vmem((3, 2, HALF, WIDTH), BF16),
        vmem((2, HALF, WIDTH), BF16),
        vmem((2, HALF, WIDTH), BF16),
        vmem((2, HALF, WIDTH), BF16),
    ]
    scratch = [
        vmem((ROWS, 512), BF16),
        vmem((512, WIDTH), BF16),
        vmem((BLOCK, WIDTH), BF16),
        vmem((1, WIDTH), F32),
        vmem((1, WIDTH), F32),
        vmem((WIDTH, COLS), BF16),
        vmem((1, COLS), F32),
        vmem((ROWS, 4), jnp.int32),
        vmem((ROWS, 4), F32),
        vmem((ROWS, WIDTH), BF16),
        vmem((ROWS, COLS), F32),
        vmem((ROWS, COLS), F32),
        vmem((ROWS, WIDTH), BF16),
        vmem((ROWS, COLS), BF16),
        vmem((BLOCK, WIDTH), F32),
        vmem((BLOCK, 128), F32),
        *rs_bufs,
        vmem((4, HALF, WIDTH), F32),
        *rs_bufs,
        vmem((ROWS, 128), F32),
        vmem((ROWS, 128), F32),
        vmem((ROWS, 128), F32),
        vmem((3, 8, 128), F32),
        vmem((6, 8, 128), F32),
        vmem((RING, 128), F32),
        vmem((2 * NSUB, CHUNK, SUB), F32),
        vmem((NZ * NSUB, CHUNK, SUB), BF16),
        vmem((NZ * NSUB, CHUNK, SUB), BF16),
        vmem(((NZ - 1) * NSUB, CHUNK, SUB), BF16),
        vmem(((NZ - 1) * NSUB, CHUNK, SUB), BF16),
        vmem((BLOCK, WIDTH), F32),
        vmem((NSUB, CHUNK, SUB), F32),
        dma((11,)),
        dma((16,)),
        dma((NSUB + 1,)),
        *[dma((30,))] * 4,
        *[dma((20,))] * 2,
        *[dma((6,))] * 2,
        *[dma((NZ * NSUB,))] * 2,
        *[dma(((NZ - 1) * NSUB,))] * 2,
    ]
    losses, stream_grad, vocab_grad = pl.pallas_call(
        kernel,
        out_shape=(
            jax.ShapeDtypeStruct((1, BLOCK), F32),
            jax.ShapeDtypeStruct((BLOCK, WIDTH), F32),
            jax.ShapeDtypeStruct((CHUNK, COLS), F32),
        ),
        in_specs=[hbm] * 9,
        out_specs=(pl.BlockSpec(memory_space=pltpu.VMEM), pl.BlockSpec(memory_space=pltpu.HBM), pl.BlockSpec(memory_space=pltpu.HBM)),
        scratch_shapes=scratch,
        compiler_params=pltpu.CompilerParams(
            collective_id=0, has_side_effects=True, vmem_limit_bytes=60 * 1024 * 1024
        ),
    )(hid, down, res, pg.reshape(1, WIDTH), fg.reshape(1, WIDTH), voc,
      bias.reshape(1, COLS), ids, wts)
    return losses.reshape(BLOCK), stream_grad, vocab_grad


def solution(mesh):
    split = Mesh(mesh.devices.reshape(4, 4, 8, 2), AXES)
    vp, dp = ("y", "x"), ("z", "c")
    return jax.shard_map(
        shards,
        mesh=split,
        in_specs=(
            P(dp, vp),
            P(vp, None),
            P(dp + vp, None),
            P(),
            P(),
            P(None, vp),
            P(vp),
            P(dp, None),
            P(dp, None),
        ),
        out_specs=(P(dp + vp), P(dp + vp, None), P(dp, vp)),
        check_vma=False,
    )
```

```python
import jax
import jax.numpy as jnp
from jax import lax
from jax.experimental import pallas as pl
from jax.experimental.pallas import tpu as pltpu
from jax.sharding import Mesh
from jax.sharding import PartitionSpec as P

MESH = pl.DeviceIdType.MESH
F32 = jnp.float32
BF16 = jnp.bfloat16
AXES = ("y", "x", "z", "c")

EPSILON = 1e-06
Z_WEIGHT = 0.001
LOSS_SCALE = 32.0

RING = 4
NZ = 8
BLOCK = 32
HALF = 16
CHUNK = 128
ROWS = 512
WIDTH = 2048
COLS = 2048
SUB = 512
NSUB = COLS // SUB
RS_ORDER = (2, 1, 3, 0)
AG_ORDER = (0, 3, 1, 2)


def inverse_rms(values):
    return lax.rsqrt(jnp.mean(values * values, axis=-1, keepdims=True) + EPSILON)


def aligned(start, size, unit):
    return pl.ds(pl.multiple_of(start, unit), size)


def kernel(
    hid, down, res, pg, fg, voc, bias, ids, wts,
    loss_o, sg_o, vg_o,
    hid_v, down_v, res_v, pg_v, fg_v, voc_v, bias_v, ids_v, wts_v, meta_v,
    part, scores, wanted, normed, grads, stream_v, inv_v,
    ra, rb, rc, sb2, ra2, rb2, rc2, keep2,
    rra, rrb, rrc, rsb2, rra2, rrb2, rrc2,
    stat_c, turn_v, norm_c, stat_s, stat_r, loss_v, loss_out,
    v_own, pair_s, pair_r, z_s, z_r, sg_v, vg_v,
    load_sem, hid_sem, out_sem,
    rs_ss, rs_rs, rr_ss, rr_rs, ag_ss, ag_rs, st_ss, st_rs, pr_ss, pr_rs, z_ss, z_rs,
):
    y, x, z, c = (lax.axis_index(name) for name in AXES)
    a = x + c * (y - x)
    b = y + c * (x - y)

    def mod4(value):
        return lax.rem(value, RING)

    def dev_a(step):
        to = mod4(a + step)
        return (y + c * (to - y), to + c * (x - to), z, c)

    def dev_b(step):
        to = mod4(b + step)
        return (to + c * (y - to), x + c * (to - x), z, c)

    up_z = lax.rem(z + 1 + c * (NZ - 2), NZ)
    down_z = lax.rem(z + NZ - 1 - c * (NZ - 2), NZ)
    dev_up = (y, x, up_z, c)
    dev_down = (y, x, down_z, c)
    dev_pair = (y, x, z, 1 - c)

    def source_row(i, q):
        return (i * (1 + 3 * c) + q * (4 - 3 * c)) * BLOCK

    def rows(i, q, h):
        return aligned(i * CHUNK + q * BLOCK + h * HALF, HALF, HALF)

    def rows32(i, q):
        return aligned(i * CHUNK + q * BLOCK, BLOCK, BLOCK)

    def chunk_rows(i):
        return aligned(i * CHUNK, CHUNK, CHUNK)

    def sub_cols(j):
        return aligned(j * SUB, SUB, SUB)

    def remote(src, dst, send, recv, to):
        return pltpu.make_async_remote_copy(
            src_ref=src, dst_ref=dst, send_sem=send, recv_sem=recv,
            device_id=to, device_id_type=MESH,
        )

    def arrived(view, sem):
        remote(view, view, sem, sem, dev_pair).wait_recv()

    def gone(view, sem):
        remote(view, view, sem, sem, dev_pair).wait_send()

    a_up, a_dn, a_far = dev_a(1), dev_a(3), dev_a(2)
    b_up, b_dn, b_far = dev_b(1), dev_b(3), dev_b(2)

    barrier = pltpu.get_barrier_semaphore()
    for to in (a_up, a_dn, a_far, b_up, b_dn, b_far, dev_pair, dev_down):
        pl.semaphore_signal(barrier, inc=1, device_id=to, device_id_type=MESH)

    hid_copies = []
    for i in range(RING):
        for q in range(RING):
            hid_copies.append(
                pltpu.make_async_copy(
                    hid.at[aligned(source_row(i, q), BLOCK, BLOCK), :],
                    hid_v.at[pl.ds(i * CHUNK + q * BLOCK, BLOCK), :],
                    hid_sem,
                )
            )
    pairs = [(down.at[:, pl.ds(k * SUB, SUB)], down_v.at[:, pl.ds(k * SUB, SUB)]) for k in range(4)]
    pairs += [
        (ids, ids_v), (wts, wts_v), (res, res_v), (pg, pg_v), (fg, fg_v), (bias, bias_v),
    ]
    pairs += [
        (voc.at[pl.ds(k * SUB, SUB), :], voc_v.at[pl.ds(k * SUB, SUB), :]) for k in range(4)
    ]
    loads = [
        pltpu.make_async_copy(src, dst, load_sem.at[min(k, 10)])
        for k, (src, dst) in enumerate(pairs)
    ]
    for copy in hid_copies + loads[0:4]:
        copy.start()

    def branch_chunk(i, send, ready=None):
        def piece(n, carry):
            value = jnp.dot(
                hid_v[chunk_rows(i), :], down_v[:, sub_cols(n)], preferred_element_type=F32
            )
            scores[chunk_rows(i), sub_cols(n)] = value
            if send:
                part[chunk_rows(i), sub_cols(n)] = value.astype(BF16)
            return carry

        if ready is None:
            lax.fori_loop(0, WIDTH // SUB, piece, 0)
        else:
            for n in range(WIDTH // SUB):
                ready[n].wait()
                piece(n, 0)

    def rs_tools(ra, rb, rc, sb2, ra2, rb2, rc2, ss, rs):
        far, up, dn = mod4(a + 2), mod4(a + 1), mod4(a + 3)

        def q_of(t):
            return mod4(b + RS_ORDER[t])

        def one(kind, t):
            q = q_of(t)
            src, dst, to = (
                (rows(far, q, 0), ra.at[0, t], a_up),
                (rows(far, q, 1), ra.at[1, t], a_dn),
                (rows(up, q, 1), rb.at[0, t], a_up),
                (rows(dn, q, 0), rb.at[1, t], a_dn),
                (rows(up, q, 0), rc.at[0, t], a_up),
                (rows(dn, q, 1), rc.at[1, t], a_dn),
            )[kind]
            recv = rs.at[t if kind < 2 else RING + t]
            return remote(part.at[src, :], dst, ss, recv, to)

        def two(kind):
            src, dst, to = (
                (sb2.at[0, 0], ra2.at[0], b_up),
                (sb2.at[0, 1], ra2.at[1], b_dn),
                (sb2.at[1, 1], rb2.at[0], b_up),
                (sb2.at[2, 0], rb2.at[1], b_dn),
                (sb2.at[1, 0], rc2.at[0], b_up),
                (sb2.at[2, 1], rc2.at[1], b_dn),
            )[kind]
            return remote(src, dst, ss, rs.at[8 + min(kind, 2)], to)

        def first():
            for t in range(RING):
                one(0, t).start()
                one(1, t).start()

        def second(t):
            one(2, t).start()
            one(3, t).start()

        def middle():
            for t in range(RING):
                q = q_of(t)
                arrived(ra.at[:, t], rs.at[t])
                for kind, i, h in ((0, up, 0), (1, dn, 1)):
                    part[rows(i, q, h), :] = (
                        scores[rows(i, q, h), :] + ra[h, t].astype(F32)
                    ).astype(BF16)
                    one(4 + kind, t).start()
                if t < 2:
                    second(t + 2)

        def finish_a(turns):
            for t in turns:
                q = q_of(t)
                arrived(part.at[pl.ds(0, 4 * HALF), :], rs.at[RING + t])
                low = scores[rows(a, q, 0), :] + rc[0, t].astype(F32) + rb[1, t].astype(F32)
                high = scores[rows(a, q, 1), :] + rb[0, t].astype(F32) + rc[1, t].astype(F32)
                if t == 0:
                    sb2[0, 0] = low.astype(BF16)
                    two(0).start()
                    sb2[0, 1] = high.astype(BF16)
                    two(1).start()
                elif t == 1:
                    sb2[1, 1] = high.astype(BF16)
                    two(2).start()
                    keep2[0] = low
                elif t == 2:
                    sb2[2, 0] = low.astype(BF16)
                    two(3).start()
                    keep2[1] = high
                else:
                    keep2[2] = low
                    keep2[3] = high

        def middle_b():
            two(0).wait_recv()
            sb2[1, 0] = (keep2[0] + ra2[0].astype(F32)).astype(BF16)
            two(4).start()
            two(1).wait_recv()
            sb2[2, 1] = (keep2[1] + ra2[1].astype(F32)).astype(BF16)
            two(5).start()

        def finish_b():
            arrived(part.at[pl.ds(0, 4 * HALF), :], rs.at[10])
            low = keep2[2] + rc2[0].astype(F32) + rb2[1].astype(F32)
            high = keep2[3] + rb2[0].astype(F32) + rc2[1].astype(F32)
            return jnp.concatenate([low, high], axis=0)

        def sent():
            gone(part.at[pl.ds(0, 30 * HALF), :], ss)

        return first, second, middle, finish_a, middle_b, finish_b, sent

    def wanted_block(p):
        i, q = p // RING, lax.rem(p, RING)
        at = aligned(source_row(i, q), BLOCK, BLOCK)
        local = meta_v[at, 0:4] - ((y * RING + x) * COLS).astype(F32)
        weight = meta_v[at, 4:8]
        for n in range(NSUB):
            position = (lax.broadcasted_iota(jnp.int32, (BLOCK, SUB), 1) + n * SUB).astype(F32)
            total = jnp.zeros((BLOCK, SUB), F32)
            for k in range(4):
                total = total + jnp.where(
                    local[:, k : k + 1] == position, weight[:, k : k + 1], 0.0
                )
            wanted[aligned(p * BLOCK, BLOCK, BLOCK), pl.ds(n * SUB, SUB)] = total

    def wanted_blocks(start, stop):
        def body(p, carry):
            wanted_block(p)
            return carry

        lax.fori_loop(start, stop, body, 0)

    first, second, middle, finish_a, middle_b, finish_b, sent = rs_tools(
        ra, rb, rc, sb2, ra2, rb2, rc2, rs_ss, rs_rs
    )
    pltpu.make_async_copy(hid, hid_v, hid_sem).wait()
    branch_chunk(mod4(a + 2), True, loads[0:4])
    for copy in loads[4:]:
        copy.start()
    pl.semaphore_wait(barrier, 8)
    first()
    branch_chunk(mod4(a + 1), True)
    branch_chunk(mod4(a + 3), True)
    second(0)
    second(1)
    branch_chunk(a, False)
    middle()
    for copy in loads[4:10]:
        copy.wait()
    for g in range(RING):
        lanes = pl.ds(g * 128, 128)
        both = jnp.concatenate([ids_v[:, lanes].astype(F32), wts_v[:, lanes]], axis=0)
        meta_v[lanes, :] = jnp.transpose(jnp.concatenate([both] * 16, axis=0))
    wanted_blocks(0, 8)
    finish_a((0,))
    wanted_blocks(8, 16)
    finish_a((1, 2))
    middle_b()
    finish_a((3,))
    branch = finish_b()

    stream = res_v[...].astype(F32) + branch * inverse_rms(branch) * pg_v[...]
    inverse = inverse_rms(stream)
    stream_v[...] = stream
    inv_v[...] = jnp.broadcast_to(inverse, inv_v.shape)
    normed[rows32(a, b), :] = (stream * inverse * fg_v[...]).astype(BF16)

    up, dn, far = mod4(a + 1), mod4(a + 3), mod4(a + 2)
    b1, b3, b2 = mod4(b + 1), mod4(b + 3), mod4(b + 2)

    def gather_b(kind, arriving=False):
        at, to = (
            (rows32(a, b3 if arriving else b), b_up),
            (rows32(a, b1 if arriving else b), b_dn),
            (rows(a, b2 if arriving else b3, 0), b_up),
            (rows(a, b2 if arriving else b1, 1), b_dn),
        )[kind]
        return remote(
            normed.at[at, :], normed.at[at, :], ag_ss.at[kind // 2], ag_rs.at[min(kind, 2)], to
        )

    def gather_a(kind, t, arriving=False):
        q = mod4(b + AG_ORDER[t])
        at, to = (
            (rows32(dn if arriving else a, q), a_up),
            (rows32(up if arriving else a, q), a_dn),
            (rows(far if arriving else dn, q, 0), a_up),
            (rows(far if arriving else up, q, 1), a_dn),
        )[kind]
        recv = ag_rs.at[3 + 2 * t + kind if kind < 2 else 11]
        return remote(normed.at[at, :], normed.at[at, :], ag_ss.at[1], recv, to)

    def forward_a(t):
        for kind in (0, 1):
            gather_a(kind, t, True).wait_recv()
            gather_a(2 + kind, t).start()

    for kind in (0, 1):
        gather_b(kind).start()
    gone(normed.at[pl.ds(0, 2 * BLOCK), :], ag_ss.at[0])
    for kind in (0, 1):
        gather_a(kind, 0).start()
    for kind in (0, 1):
        gather_b(kind, True).wait_recv()
        gather_b(2 + kind).start()
    for kind in (0, 1):
        gather_a(0, 1 + kind).start()
        gather_a(1, 1 + kind).start()
    forward_a(0)
    arrived(normed.at[rows32(a, b2), :], ag_rs.at[2])
    for kind in (0, 1):
        gather_a(kind, 3).start()
    pltpu.make_async_copy(voc, voc_v, load_sem.at[10]).wait()

    def score_pieces(chunks, start, stop):
        def piece(n, carry):
            rows_in = [normed[chunk_rows(i), :] for i in chunks]
            value = jnp.dot(
                jnp.concatenate(rows_in, axis=0), voc_v[:, sub_cols(n)], preferred_element_type=F32
            ) + bias_v[:, sub_cols(n)]
            for k, i in enumerate(chunks):
                scores[chunk_rows(i), sub_cols(n)] = value[k * CHUNK : (k + 1) * CHUNK]
            return carry

        lax.fori_loop(start, stop, piece, 0)

    first_lane = lax.broadcasted_iota(jnp.int32, (64, 128), 1) == 0

    def stats(i):
        for r in range(2):
            at = aligned(i * CHUNK + r * 64, 64, 64)
            groups = [pl.ds(g * 128, 128) for g in range(COLS // 128)]
            peak = scores[at, groups[0]]
            for group in groups[1:]:
                peak = jnp.maximum(peak, scores[at, group])
            peak = jnp.broadcast_to(jnp.max(peak, axis=1, keepdims=True), (64, 128))
            total = jnp.zeros((64, 128), F32)
            target = jnp.zeros((64, 128), F32)
            for group in groups:
                value = scores[at, group]
                total = total + jnp.exp(value - peak)
                target = target + wanted[at, group] * value
            lse = peak + jnp.log(jnp.sum(total, axis=1, keepdims=True))
            stat_c[pl.ds(r * 64, 64), :] = jnp.where(
                first_lane, lse, jnp.sum(target, axis=1, keepdims=True)
            )
        turned = jnp.transpose(stat_c[...])
        stat_s[0, pl.ds(i, 1), :] = turned[0:1, :]
        stat_s[0, pl.ds(i + RING, 1), :] = turned[1:2, :]

    score_pieces((a,), 0, 2)
    forward_a(1)
    score_pieces((a,), 2, 4)
    forward_a(2)
    stats(a)
    forward_a(3)
    score_pieces((up, dn), 0, 4)
    stats(up)
    stats(dn)
    arrived(normed.at[chunk_rows(far), :], ag_rs.at[11])
    score_pieces((far,), 0, 4)
    stats(far)

    def stat_copy(phase, k):
        to = ((a_up, a_dn, a_far), (b_up, b_dn, b_far))[phase][k]
        n = phase * 3 + k
        return remote(stat_s.at[phase], stat_r.at[n], st_ss, st_rs.at[phase], to)

    def vocab_rows(s):
        away = (1 - 2 * c) * (1 + s)
        own_dest = lax.rem(z + 2 * NZ - away, NZ) * 2 + c
        pair_dest = lax.rem(z + 2 * NZ + away, NZ) * 2 + 1 - c
        return jnp.concatenate(
            [normed[:, aligned(dest * CHUNK, CHUNK, CHUNK)] for dest in (own_dest, pair_dest)], axis=1
        )

    is_lse = lax.broadcasted_iota(jnp.int32, (8, 128), 0) < RING
    for phase in range(2):
        for k in range(3):
            stat_copy(phase, k).start()
        if phase == 0:
            turn_v[...] = jnp.transpose(vocab_rows(0))
        arrived(stat_r.at[pl.ds(phase * 3, 3)], st_rs.at[phase])
        parts = [stat_s[phase]] + [stat_r[phase * 3 + k] for k in range(3)]
        peak = jnp.maximum(jnp.maximum(parts[0], parts[1]), jnp.maximum(parts[2], parts[3]))
        joint = peak + jnp.log(sum(jnp.exp(value - peak) for value in parts))
        stat_s[phase + 1] = jnp.where(is_lse, joint, sum(parts))
    log_rows = stat_s[2, 0:RING, :]
    for i in range(RING):
        norm_c[pl.ds(i * CHUNK, CHUNK), :] = jnp.transpose(
            jnp.broadcast_to(stat_s[2, i : i + 1, :], (CHUNK, 128))
        )
    loss_v[...] = log_rows - stat_s[2, RING:8, :] + Z_WEIGHT * log_rows * log_rows

    def grad_block(j):
        def body(r, carry):
            at = aligned(r * 64, 64, 64)
            log_norm = norm_c[at, :]
            factor = 1.0 + 2.0 * Z_WEIGHT * log_norm
            for n in range(SUB // 128):
                cols = aligned(j * SUB + n * 128, 128, 128)
                probability = jnp.exp(scores[at, cols] - log_norm)
                grads[at, cols] = (
                    LOSS_SCALE * (probability * factor - wanted[at, cols])
                ).astype(BF16)
            return carry

        lax.fori_loop(0, ROWS // 64, body, 0)

    def pair_copy(s, j):
        k = s * NSUB + j
        return remote(pair_s.at[k], pair_r.at[k], pr_ss, pr_rs.at[k], dev_pair)

    def z_copy(s, j):
        k = s * NSUB + j
        return remote(z_s.at[k], z_r.at[k], z_ss, z_rs.at[k], dev_up)

    def vocab_piece(s, j):
        if s == 0:
            value = jnp.dot(turn_v[...], grads[:, sub_cols(j)], preferred_element_type=F32)
        else:
            value = lax.dot_general(
                vocab_rows(s), grads[:, sub_cols(j)], (((0,), (0,)), ((), ())),
                preferred_element_type=F32,
            )
        v_own[(s % 2) * NSUB + j] = value[0:CHUNK]
        pair_s[s * NSUB + j] = value[CHUNK:].astype(BF16)
        pair_copy(s, j).start()

    def z_piece(s, j):
        k = s * NSUB + j
        pair_copy(s, j).wait_recv()
        value = v_own[(s % 2) * NSUB + j] + pair_r[k].astype(F32)
        if s > 0:
            z_copy(s - 1, j).wait_recv()
            value = value + z_r[k - NSUB].astype(F32)
        if s < NZ - 1:
            z_s[k] = value.astype(BF16)
            z_copy(s, j).start()
        else:
            vg_v[j] = value
            out_copy(j).start()

    def out_copy(j):
        return pltpu.make_async_copy(vg_v.at[j], vg_o.at[:, sub_cols(j)], out_sem.at[j])

    def row_piece(i, n):
        value = lax.dot_general(
            grads[chunk_rows(i), :], voc_v[sub_cols(n), :],
            (((1,), (1,)), ((), ())), preferred_element_type=F32,
        )
        scores[chunk_rows(i), sub_cols(n)] = value
        part[chunk_rows(i), sub_cols(n)] = value.astype(BF16)

    for j in range(NSUB):
        grad_block(j)
        vocab_piece(0, j)
        if j > 0:
            z_piece(0, j - 1)
    z_piece(0, NSUB - 1)
    sent()

    first, second, middle, finish_a, middle_b, finish_b, sent_rows = rs_tools(
        rra, rrb, rrc, rsb2, rra2, rrb2, rrc2, rr_ss, rr_rs
    )
    def drain():
        sent_rows()
        gone(normed.at[pl.ds(0, 26 * HALF), :], ag_ss.at[1])
        gone(stat_r, st_ss)
        gone(pair_s, pr_ss)

    row_order = (far, up, dn, a)
    for s in range(NZ):

        def slot(j, carry):
            if s > 0:
                z_piece(s, j)
            if s < NZ - 1:
                vocab_piece(s + 1, j)
            if s < RING:
                row_piece(row_order[s], j)
            return carry

        lax.fori_loop(0, NSUB, slot, 0)
        if s == 0:
            first()
        elif s == 2:
            second(0)
            second(1)
            middle()
        elif s == 4:
            finish_a(range(RING))
        elif s == 5:
            middle_b()
        elif s == 6:
            stream = stream_v[...]
            inverse = inv_v[:, 0:1]
            upstream = finish_b() * fg_v[...]
            sg_v[...] = inverse * (
                upstream
                - stream * inverse * inverse * jnp.mean(upstream * stream, axis=-1, keepdims=True)
            )
            pltpu.make_async_copy(sg_v, sg_o, out_sem.at[NSUB]).start()
            own = jnp.broadcast_to(loss_v[pl.ds(a, 1), :], (8, 128))
            own = pltpu.roll(own, lax.rem(128 - b * BLOCK, 128), 1)
            loss_out[...] = own[0:1, 0:BLOCK]
            pltpu.make_async_copy(loss_out, loss_o, out_sem.at[NSUB + 1]).start()
            drain()

    gone(z_s, z_ss)
    for j in range(NSUB):
        out_copy(j).wait()
    pltpu.make_async_copy(sg_v, sg_o, out_sem.at[NSUB]).wait()
    pltpu.make_async_copy(loss_out, loss_o, out_sem.at[NSUB + 1]).wait()


def shards(hid, down, res, pg, fg, voc, bias, ids, wts):
    hbm = pl.BlockSpec(memory_space=pl.ANY)
    vmem = pltpu.VMEM
    dma = pltpu.SemaphoreType.DMA
    rs_bufs = [
        vmem((2, RING, HALF, WIDTH), BF16),
        vmem((2, RING, HALF, WIDTH), BF16),
        vmem((2, RING, HALF, WIDTH), BF16),
        vmem((3, 2, HALF, WIDTH), BF16),
        vmem((2, HALF, WIDTH), BF16),
        vmem((2, HALF, WIDTH), BF16),
        vmem((2, HALF, WIDTH), BF16),
    ]
    scratch = [
        vmem((ROWS, 512), BF16),
        vmem((512, WIDTH), BF16),
        vmem((BLOCK, WIDTH), BF16),
        vmem((1, WIDTH), F32),
        vmem((1, WIDTH), F32),
        vmem((WIDTH, COLS), BF16),
        vmem((1, COLS), F32),
        vmem((4, ROWS), jnp.int32),
        vmem((4, ROWS), F32),
        vmem((ROWS, 128), F32),
        vmem((ROWS, WIDTH), BF16),
        vmem((ROWS, COLS), F32),
        vmem((ROWS, COLS), F32),
        vmem((ROWS, WIDTH), BF16),
        vmem((ROWS, COLS), BF16),
        vmem((BLOCK, WIDTH), F32),
        vmem((BLOCK, 128), F32),
        *rs_bufs,
        vmem((4, HALF, WIDTH), F32),
        *rs_bufs,
        vmem((CHUNK, 128), F32),
        vmem((2 * CHUNK, ROWS), BF16),
        vmem((ROWS, 128), F32),
        vmem((3, 8, 128), F32),
        vmem((6, 8, 128), F32),
        vmem((RING, 128), F32),
        vmem((1, BLOCK), F32),
        vmem((2 * NSUB, CHUNK, SUB), F32),
        vmem((NZ * NSUB, CHUNK, SUB), BF16),
        vmem((NZ * NSUB, CHUNK, SUB), BF16),
        vmem(((NZ - 1) * NSUB, CHUNK, SUB), BF16),
        vmem(((NZ - 1) * NSUB, CHUNK, SUB), BF16),
        vmem((BLOCK, WIDTH), F32),
        vmem((NSUB, CHUNK, SUB), F32),
        dma((11,)),
        dma(()),
        dma((NSUB + 2,)),
        dma(()), dma((11,)), dma(()), dma((11,)),
        dma((2,)), dma((12,)),
        dma(()), dma((2,)),
        dma(()), dma((NZ * NSUB,)),
        dma(()), dma(((NZ - 1) * NSUB,)),
    ]
    losses, stream_grad, vocab_grad = pl.pallas_call(
        kernel,
        out_shape=(
            jax.ShapeDtypeStruct((1, BLOCK), F32),
            jax.ShapeDtypeStruct((BLOCK, WIDTH), F32),
            jax.ShapeDtypeStruct((CHUNK, COLS), F32),
        ),
        in_specs=[hbm] * 9,
        out_specs=(hbm,) * 3,
        scratch_shapes=scratch,
        compiler_params=pltpu.CompilerParams(
            collective_id=0, has_side_effects=True, vmem_limit_bytes=60 * 1024 * 1024
        ),
    )(hid, down, res, pg.reshape(1, WIDTH), fg.reshape(1, WIDTH), voc,
      bias.reshape(1, COLS), ids.T, wts.T)
    blocks = (
        pl.BlockSpec((1, BLOCK), lambda g: (0, 0)),
        pl.BlockSpec((BLOCK // 2, WIDTH), lambda g: (g, 0)),
        pl.BlockSpec((CHUNK // 2, COLS), lambda g: (g, 0)),
    )

    def place(*refs):
        for k in range(3):
            refs[3 + k][...] = refs[k][...]

    losses, stream_grad, vocab_grad = pl.pallas_call(
        place,
        grid=(2,),
        out_shape=tuple(jax.ShapeDtypeStruct(o.shape, o.dtype) for o in (losses, stream_grad, vocab_grad)),
        in_specs=blocks,
        out_specs=blocks,
    )(losses, stream_grad, vocab_grad)
    return losses.reshape(BLOCK), stream_grad, vocab_grad


def solution(mesh):
    split = Mesh(mesh.devices.reshape(4, 4, 8, 2), AXES)
    vp, dp = ("y", "x"), ("z", "c")
    return jax.shard_map(
        shards,
        mesh=split,
        in_specs=(
            P(dp, vp),
            P(vp, None),
            P(dp + vp, None),
            P(),
            P(),
            P(None, vp),
            P(vp),
            P(dp, None),
            P(dp, None),
        ),
        out_specs=(P(dp + vp), P(dp + vp, None), P(dp, vp)),
        check_vma=False,
    )
```

```python
import jax
import jax.numpy as jnp
from jax import lax
from jax.experimental import pallas as pl
from jax.experimental.pallas import tpu as pltpu
from jax.sharding import Mesh
from jax.sharding import PartitionSpec as P

MESH = pl.DeviceIdType.MESH
F32 = jnp.float32
BF16 = jnp.bfloat16
AXES = ("y", "x", "z", "c")

EPSILON = 1e-06
Z_WEIGHT = 0.001
LOSS_SCALE = 32.0

RING = 4
NZ = 8
BLOCK = 32
HALF = 16
CHUNK = 128
ROWS = 512
WIDTH = 2048
COLS = 2048
SUB = 512
NSUB = COLS // SUB
RS_ORDER = (2, 1, 3, 0)
AG_ORDER = (0, 3, 1, 2)


def inverse_rms(values):
    return lax.rsqrt(jnp.mean(values * values, axis=-1, keepdims=True) + EPSILON)


def aligned(start, size, unit):
    return pl.ds(pl.multiple_of(start, unit), size)


def kernel(
    hid, down, res, pg, fg, voc, bias, ids, wts,
    loss_o, sg_o, vg_o,
    hid_v, down_v, res_v, pg_v, fg_v, voc_v, bias_v, ids_v, wts_v, meta_v,
    part, scores, wanted, normed, grads, stream_v, inv_v,
    ra, rb, rc, sb2, ra2, rb2, rc2, keep2,
    rra, rrb, rrc, rsb2, rra2, rrb2, rrc2,
    stat_c, turn_v, norm_c, stat_s, stat_r, loss_v,
    v_own, pair_s, pair_r, z_s, z_r,
    load_sem, hid_sem,
    rs_ss, rs_rs, rr_ss, rr_rs, ag_ss, ag_rs, st_ss, st_rs, pr_ss, pr_rs, z_ss, z_rs,
):
    y, x, z, c = (lax.axis_index(name) for name in AXES)
    a = x + c * (y - x)
    b = y + c * (x - y)

    def mod4(value):
        return lax.rem(value, RING)

    def dev(step_a, step_b):
        to_a, to_b = mod4(a + step_a), mod4(b + step_b)
        return (to_b + c * (to_a - to_b), to_a + c * (to_b - to_a), z, c)

    up_z = lax.rem(z + 1 + c * (NZ - 2), NZ)
    down_z = lax.rem(z + NZ - 1 - c * (NZ - 2), NZ)
    dev_up = (y, x, up_z, c)
    dev_down = (y, x, down_z, c)
    dev_pair = (y, x, z, 1 - c)

    def source_row(i, q):
        return (i * (1 + 3 * c) + q * (4 - 3 * c)) * BLOCK

    def rows(i, q, h):
        return aligned(i * CHUNK + q * BLOCK + h * HALF, HALF, HALF)

    def rows32(i, q):
        return aligned(i * CHUNK + q * BLOCK, BLOCK, BLOCK)

    def chunk_rows(i):
        return aligned(i * CHUNK, CHUNK, CHUNK)

    def sub_cols(j):
        return aligned(j * SUB, SUB, SUB)

    def remote(src, dst, send, recv, to):
        return pltpu.make_async_remote_copy(
            src_ref=src, dst_ref=dst, send_sem=send, recv_sem=recv,
            device_id=to, device_id_type=MESH,
        )

    def arrived(view, sem):
        remote(view, view, sem, sem, dev_pair).wait_recv()

    def gone(view, sem):
        remote(view, view, sem, sem, dev_pair).wait_send()

    a_up, a_dn, b_up, b_dn = dev(1, 0), dev(3, 0), dev(0, 1), dev(0, 3)

    barrier = pltpu.get_barrier_semaphore()
    for to in (a_up, a_dn, b_up, b_dn, dev_pair, dev_down):
        pl.semaphore_signal(barrier, inc=1, device_id=to, device_id_type=MESH)

    hid_copies = []
    for i in range(RING):
        for q in range(RING):
            hid_copies.append(
                pltpu.make_async_copy(
                    hid.at[aligned(source_row(i, q), BLOCK, BLOCK), :],
                    hid_v.at[pl.ds(i * CHUNK + q * BLOCK, BLOCK), :],
                    hid_sem,
                )
            )
    pairs = [(down.at[:, pl.ds(k * SUB, SUB)], down_v.at[:, pl.ds(k * SUB, SUB)]) for k in range(4)]
    pairs += [
        (ids, ids_v), (wts, wts_v), (res, res_v), (pg, pg_v), (fg, fg_v), (bias, bias_v),
    ]
    pairs += [
        (voc.at[pl.ds(k * SUB, SUB), :], voc_v.at[pl.ds(k * SUB, SUB), :]) for k in range(4)
    ]
    loads = [
        pltpu.make_async_copy(src, dst, load_sem.at[min(k, 10)])
        for k, (src, dst) in enumerate(pairs)
    ]
    for copy in hid_copies + loads[0:4]:
        copy.start()

    def branch_chunk(i, send, ready=None):
        def piece(n, carry):
            value = jnp.dot(
                hid_v[chunk_rows(i), :], down_v[:, sub_cols(n)], preferred_element_type=F32
            )
            if ready is None:
                scores[chunk_rows(i), sub_cols(n)] = value
            if send:
                part[chunk_rows(i), sub_cols(n)] = value.astype(BF16)
            return carry

        if ready is None:
            lax.fori_loop(0, WIDTH // SUB, piece, 0)
        else:
            for n in range(WIDTH // SUB):
                ready[n].wait()
                piece(n, 0)

    def rs_tools(ra, rb, rc, sb2, ra2, rb2, rc2, ss, rs):
        far, up, dn = mod4(a + 2), mod4(a + 1), mod4(a + 3)

        def q_of(t):
            return mod4(b + RS_ORDER[t])

        def one(kind, t):
            q = q_of(t)
            src, dst, to = (
                (rows(far, q, 0), ra.at[0, t], a_up),
                (rows(far, q, 1), ra.at[1, t], a_dn),
                (rows(up, q, 1), rb.at[0, t], a_up),
                (rows(dn, q, 0), rb.at[1, t], a_dn),
                (rows(up, q, 0), rc.at[0, t], a_up),
                (rows(dn, q, 1), rc.at[1, t], a_dn),
            )[kind]
            recv = rs.at[t if kind < 2 else RING + t]
            return remote(part.at[src, :], dst, ss, recv, to)

        def two(kind):
            src, dst, to = (
                (sb2.at[0, 0], ra2.at[0], b_up),
                (sb2.at[0, 1], ra2.at[1], b_dn),
                (sb2.at[1, 1], rb2.at[0], b_up),
                (sb2.at[2, 0], rb2.at[1], b_dn),
                (sb2.at[1, 0], rc2.at[0], b_up),
                (sb2.at[2, 1], rc2.at[1], b_dn),
            )[kind]
            return remote(src, dst, ss, rs.at[8 + min(kind, 2)], to)

        def first(turns):
            for t in turns:
                one(0, t).start()
                one(1, t).start()

        def second(turns):
            for t in turns:
                one(2, t).start()
                one(3, t).start()

        def third(turns):
            for t in turns:
                q = q_of(t)
                arrived(ra.at[:, t], rs.at[t])
                for kind, i, h in ((0, up, 0), (1, dn, 1)):
                    part[rows(i, q, h), :] = (
                        scores[rows(i, q, h), :] + ra[h, t].astype(F32)
                    ).astype(BF16)
                    one(4 + kind, t).start()

        def finish_a(turns):
            for t in turns:
                q = q_of(t)
                arrived(part.at[pl.ds(0, 4 * HALF), :], rs.at[RING + t])
                low = scores[rows(a, q, 0), :] + rc[0, t].astype(F32) + rb[1, t].astype(F32)
                high = scores[rows(a, q, 1), :] + rb[0, t].astype(F32) + rc[1, t].astype(F32)
                if t == 0:
                    sb2[0, 0] = low.astype(BF16)
                    two(0).start()
                    sb2[0, 1] = high.astype(BF16)
                    two(1).start()
                elif t == 1:
                    sb2[1, 1] = high.astype(BF16)
                    two(2).start()
                    keep2[0] = low
                elif t == 2:
                    sb2[2, 0] = low.astype(BF16)
                    two(3).start()
                    keep2[1] = high
                else:
                    keep2[2] = low
                    keep2[3] = high

        def middle_b():
            two(0).wait_recv()
            sb2[1, 0] = (keep2[0] + ra2[0].astype(F32)).astype(BF16)
            two(4).start()
            two(1).wait_recv()
            sb2[2, 1] = (keep2[1] + ra2[1].astype(F32)).astype(BF16)
            two(5).start()

        def finish_b():
            arrived(part.at[pl.ds(0, 4 * HALF), :], rs.at[10])
            low = keep2[2] + rc2[0].astype(F32) + rb2[1].astype(F32)
            high = keep2[3] + rb2[0].astype(F32) + rc2[1].astype(F32)
            return jnp.concatenate([low, high], axis=0)

        def sent():
            gone(part.at[pl.ds(0, 30 * HALF), :], ss)

        return first, second, third, finish_a, middle_b, finish_b, sent

    def wanted_block(p):
        i, q = p // RING, lax.rem(p, RING)
        at = aligned(source_row(i, q), BLOCK, BLOCK)
        local = meta_v[at, 0:4] - ((y * RING + x) * COLS).astype(F32)
        weight = meta_v[at, 4:8]
        for n in range(NSUB):
            position = (lax.broadcasted_iota(jnp.int32, (BLOCK, SUB), 1) + n * SUB).astype(F32)
            total = jnp.zeros((BLOCK, SUB), F32)
            for k in range(4):
                total = total + jnp.where(
                    local[:, k : k + 1] == position, weight[:, k : k + 1], 0.0
                )
            wanted[aligned(p * BLOCK, BLOCK, BLOCK), pl.ds(n * SUB, SUB)] = total

    def wanted_blocks(start, stop):
        def body(p, carry):
            wanted_block(p)
            return carry

        lax.fori_loop(start, stop, body, 0)

    first, second, third, finish_a, middle_b, finish_b, sent = rs_tools(
        ra, rb, rc, sb2, ra2, rb2, rc2, rs_ss, rs_rs
    )
    pltpu.make_async_copy(hid, hid_v, hid_sem).wait()
    branch_chunk(mod4(a + 2), True, loads[0:4])
    for copy in loads[4:]:
        copy.start()
    pl.semaphore_wait(barrier, 6)
    first((0, 1, 2))
    branch_chunk(mod4(a + 1), True)
    branch_chunk(mod4(a + 3), True)
    second((0, 1))
    branch_chunk(a, False)
    third((0,))
    first((3,))
    third((1,))
    second((2,))
    third((2,))
    second((3,))
    for copy in loads[4:10]:
        copy.wait()
    for g in range(RING):
        lanes = pl.ds(g * 128, 128)
        both = jnp.concatenate([ids_v[:, lanes].astype(F32), wts_v[:, lanes]], axis=0)
        meta_v[lanes, :] = jnp.transpose(jnp.concatenate([both] * 16, axis=0))
    wanted_blocks(0, 8)
    finish_a((0,))
    third((3,))
    wanted_blocks(8, 16)
    finish_a((1, 2))
    middle_b()
    finish_a((3,))
    branch = finish_b()

    stream = res_v[...].astype(F32) + branch * inverse_rms(branch) * pg_v[...]
    inverse = inverse_rms(stream)
    stream_v[...] = stream
    inv_v[...] = jnp.broadcast_to(inverse, inv_v.shape)
    normed[rows32(a, b), :] = (stream * inverse * fg_v[...]).astype(BF16)

    up, dn, far = mod4(a + 1), mod4(a + 3), mod4(a + 2)
    b1, b3, b2 = mod4(b + 1), mod4(b + 3), mod4(b + 2)

    def gather_b(kind):
        at, to = (
            (rows(a, b, 0), b_up),
            (rows(a, b, 1), b_dn),
            (rows(a, b, 1), b_up),
            (rows(a, b, 0), b_dn),
            (rows(a, b3, 0), b_up),
            (rows(a, b1, 1), b_dn),
        )[kind]
        send, recv = ((0, 0), (0, 1), (0, 2), (0, 2), (1, 3), (1, 3))[kind]
        return remote(normed.at[at, :], normed.at[at, :], ag_ss.at[send], ag_rs.at[recv], to)

    def gather_a(kind, t):
        q = mod4(b + AG_ORDER[t])
        at, to = (
            (rows32(a, q), a_up),
            (rows32(a, q), a_dn),
            (rows(dn, q, 0), a_up),
            (rows(up, q, 1), a_dn),
            (rows(a, q, 0), a_up),
            (rows(a, q, 1), a_dn),
            (rows(a, q, 1), a_up),
            (rows(a, q, 0), a_dn),
        )[kind]
        recv = ag_rs.at[(4 + 2 * t, 5 + 2 * t, 12, 12, 10, 11, 13, 13)[kind]]
        return remote(normed.at[at, :], normed.at[at, :], ag_ss.at[1], recv, to)

    def forward_a(t):
        q = mod4(b + AG_ORDER[t])
        for kind, i in ((0, dn), (1, up)):
            at = rows32(i, q) if t < 3 else rows(i, q, kind)
            arrived(normed.at[at, :], ag_rs.at[4 + 2 * t + kind])
            gather_a(2 + kind, t).start()

    for kind in range(4):
        gather_b(kind).start()

    def first_a():
        gone(normed.at[pl.ds(0, 2 * BLOCK), :], ag_ss.at[0])
        for kind in (0, 1):
            gather_a(kind, 0).start()

    pl.when(c == 0)(first_a)
    for kind, q in ((0, b3), (1, b1)):
        arrived(normed.at[rows(a, q, kind), :], ag_rs.at[kind])
        gather_b(4 + kind).start()
    pl.when(c == 1)(first_a)
    arrived(normed.at[pl.ds(0, BLOCK), :], ag_rs.at[2])
    for kind in (0, 1):
        gather_a(0, 1 + kind).start()
        gather_a(1, 1 + kind).start()
    forward_a(0)
    arrived(normed.at[rows32(a, b2), :], ag_rs.at[3])
    for kind in (4, 5, 6, 7):
        gather_a(kind, 3).start()
    pltpu.make_async_copy(voc, voc_v, load_sem.at[10]).wait()

    def score_pieces(places, start, stop):
        def piece(n, carry):
            rows_in = [normed[at, :] for at in places]
            value = jnp.dot(
                jnp.concatenate(rows_in, axis=0), voc_v[:, sub_cols(n)], preferred_element_type=F32
            ) + bias_v[:, sub_cols(n)]
            first_row = 0
            for at in places:
                scores[at, sub_cols(n)] = value[first_row : first_row + at.size]
                first_row += at.size
            return carry

        lax.fori_loop(start, stop, piece, 0)

    def stats(places):
        groups = [pl.ds(g * 128, 128) for g in range(COLS // 128)]
        for at in places:
            peak = scores[at, groups[0]]
            for group in groups[1:]:
                peak = jnp.maximum(peak, scores[at, group])
            peak = jnp.broadcast_to(jnp.max(peak, axis=1, keepdims=True), (at.size, 128))
            total = jnp.zeros((at.size, 128), F32)
            target = jnp.zeros((at.size, 128), F32)
            for group in groups:
                value = scores[at, group]
                total = total + jnp.exp(value - peak)
                target = target + wanted[at, group] * value
            lse = peak + jnp.log(jnp.sum(total, axis=1, keepdims=True))
            first_lane = lax.broadcasted_iota(jnp.int32, (at.size, 128), 1) == 0
            stat_c[at, :] = jnp.where(first_lane, lse, jnp.sum(target, axis=1, keepdims=True))

    def rows64(i):
        return [aligned(i * CHUNK + r * 64, 64, 64) for r in range(2)]

    early = [rows32(i, mod4(b + AG_ORDER[t])) for i in (up, dn) for t in range(3)]
    late = [rows32(up, b2), rows32(dn, b2)]
    score_pieces([chunk_rows(a)], 0, 2)
    forward_a(1)
    score_pieces([chunk_rows(a)], 2, 4)
    forward_a(2)
    score_pieces(early, 0, 2)
    forward_a(3)
    score_pieces(early, 2, 4)
    stats(rows64(a))
    stats(early)
    arrived(normed.at[rows32(a, b), :], ag_rs.at[13])
    arrived(normed.at[chunk_rows(far), :], ag_rs.at[12])
    score_pieces(late + [chunk_rows(far)], 0, 4)
    stats(late + rows64(far))
    for i in range(RING):
        turned = jnp.transpose(stat_c[pl.ds(i * CHUNK, CHUNK), :])
        stat_s[0, i : i + 1, :] = turned[0:1, :]
        stat_s[0, i + RING : i + RING + 1, :] = turned[1:2, :]

    def stat_copy(k):
        return remote(stat_s.at[0], stat_r.at[k], st_ss, st_rs, dev(k // RING, k % RING))

    def vocab_rows(s):
        away = (1 - 2 * c) * (1 + s)
        own_dest = lax.rem(z + 2 * NZ - away, NZ) * 2 + c
        pair_dest = lax.rem(z + 2 * NZ + away, NZ) * 2 + 1 - c
        return jnp.concatenate(
            [normed[:, aligned(dest * CHUNK, CHUNK, CHUNK)] for dest in (own_dest, pair_dest)], axis=1
        )

    is_lse = lax.broadcasted_iota(jnp.int32, (8, 128), 0) < RING
    for k in (10, 9, 11, 6, 14, 5, 7, 13, 15, 2, 8, 1, 3, 4, 12):
        stat_copy(k).start()
    turn_v[...] = jnp.transpose(vocab_rows(0))
    arrived(stat_r.at[pl.ds(1, 15)], st_rs)
    parts = [stat_s[0]] + [stat_r[k] for k in range(1, 16)]
    peak = parts[0]
    for value in parts[1:]:
        peak = jnp.maximum(peak, value)
    joint = peak + jnp.log(sum(jnp.exp(value - peak) for value in parts))
    stat_s[1] = jnp.where(is_lse, joint, sum(parts))
    log_rows = stat_s[1, 0:RING, :]
    for i in range(RING):
        norm_c[pl.ds(i * CHUNK, CHUNK), :] = jnp.transpose(
            jnp.broadcast_to(stat_s[1, i : i + 1, :], (CHUNK, 128))
        )
    loss_v[...] = log_rows - stat_s[1, RING:8, :] + Z_WEIGHT * log_rows * log_rows

    def grad_block(j):
        def body(r, carry):
            at = aligned(r * 64, 64, 64)
            log_norm = norm_c[at, :]
            factor = 1.0 + 2.0 * Z_WEIGHT * log_norm
            for n in range(SUB // 128):
                cols = aligned(j * SUB + n * 128, 128, 128)
                probability = jnp.exp(scores[at, cols] - log_norm)
                grads[at, cols] = (
                    LOSS_SCALE * (probability * factor - wanted[at, cols])
                ).astype(BF16)
            return carry

        lax.fori_loop(0, ROWS // 64, body, 0)

    def pair_copy(s, j):
        k = s * NSUB + j
        return remote(pair_s.at[k], pair_r.at[k], pr_ss, pr_rs.at[k], dev_pair)

    def z_copy(s, j):
        k = s * NSUB + j
        return remote(z_s.at[k], z_r.at[k], z_ss, z_rs.at[k], dev_up)

    def vocab_piece(s, j):
        if s == 0:
            value = jnp.dot(turn_v[...], grads[:, sub_cols(j)], preferred_element_type=F32)
        else:
            value = lax.dot_general(
                vocab_rows(s), grads[:, sub_cols(j)], (((0,), (0,)), ((), ())),
                preferred_element_type=F32,
            )
        v_own[(s % 2) * NSUB + j] = value[0:CHUNK]
        pair_s[s * NSUB + j] = value[CHUNK:].astype(BF16)
        pair_copy(s, j).start()

    def z_piece(s, j):
        k = s * NSUB + j
        pair_copy(s, j).wait_recv()
        value = v_own[(s % 2) * NSUB + j] + pair_r[k].astype(F32)
        if s > 0:
            z_copy(s - 1, j).wait_recv()
            value = value + z_r[k - NSUB].astype(F32)
        if s < NZ - 1:
            z_s[k] = value.astype(BF16)
            z_copy(s, j).start()
        else:
            vg_o[:, sub_cols(j)] = value

    def row_piece(i, n):
        value = lax.dot_general(
            grads[chunk_rows(i), :], voc_v[sub_cols(n), :],
            (((1,), (1,)), ((), ())), preferred_element_type=F32,
        )
        scores[chunk_rows(i), sub_cols(n)] = value
        part[chunk_rows(i), sub_cols(n)] = value.astype(BF16)

    for j in range(NSUB):
        grad_block(j)
        vocab_piece(0, j)
        if j > 0:
            z_piece(0, j - 1)
    z_piece(0, NSUB - 1)
    sent()

    first, second, third, finish_a, middle_b, finish_b, sent_rows = rs_tools(
        rra, rrb, rrc, rsb2, rra2, rrb2, rrc2, rr_ss, rr_rs
    )
    def drain():
        sent_rows()
        gone(normed.at[pl.ds(0, 26 * HALF), :], ag_ss.at[1])
        gone(stat_r.at[pl.ds(1, 15)], st_ss)
        gone(pair_s, pr_ss)

    row_order = (far, up, dn, a)
    for s in range(NZ):

        def slot(j, carry):
            if s > 0:
                z_piece(s, j)
            if s < NZ - 1:
                vocab_piece(s + 1, j)
            if s < RING:
                row_piece(row_order[s], j)
            return carry

        lax.fori_loop(0, NSUB, slot, 0)
        if s == 0:
            first(range(RING))
        elif s == 2:
            second((0, 1))
            third((0,))
            second((2,))
            third((1,))
            second((3,))
            third((2, 3))
        elif s == 4:
            finish_a(range(RING))
        elif s == 5:
            middle_b()
        elif s == 6:
            stream = stream_v[...]
            inverse = inv_v[:, 0:1]
            upstream = finish_b() * fg_v[...]
            sg_o[...] = inverse * (
                upstream
                - stream * inverse * inverse * jnp.mean(upstream * stream, axis=-1, keepdims=True)
            )
            own = jnp.broadcast_to(loss_v[pl.ds(a, 1), :], (8, 128))
            own = pltpu.roll(own, lax.rem(128 - b * BLOCK, 128), 1)
            loss_o[...] = own[0:1, 0:BLOCK]
            drain()

    gone(z_s, z_ss)


def shards(hid, down, res, pg, fg, voc, bias, ids, wts):
    hbm = pl.BlockSpec(memory_space=pl.ANY)
    vmem = pltpu.VMEM
    dma = pltpu.SemaphoreType.DMA
    rs_bufs = [
        vmem((2, RING, HALF, WIDTH), BF16),
        vmem((2, RING, HALF, WIDTH), BF16),
        vmem((2, RING, HALF, WIDTH), BF16),
        vmem((3, 2, HALF, WIDTH), BF16),
        vmem((2, HALF, WIDTH), BF16),
        vmem((2, HALF, WIDTH), BF16),
        vmem((2, HALF, WIDTH), BF16),
    ]
    scratch = [
        vmem((ROWS, 512), BF16),
        vmem((512, WIDTH), BF16),
        vmem((BLOCK, WIDTH), BF16),
        vmem((1, WIDTH), F32),
        vmem((1, WIDTH), F32),
        vmem((WIDTH, COLS), BF16),
        vmem((1, COLS), F32),
        vmem((4, ROWS), jnp.int32),
        vmem((4, ROWS), F32),
        vmem((ROWS, 128), F32),
        vmem((ROWS, WIDTH), BF16),
        vmem((ROWS, COLS), F32),
        vmem((ROWS, COLS), F32),
        vmem((ROWS, WIDTH), BF16),
        vmem((ROWS, COLS), BF16),
        vmem((BLOCK, WIDTH), F32),
        vmem((BLOCK, 128), F32),
        *rs_bufs,
        vmem((4, HALF, WIDTH), F32),
        *rs_bufs,
        vmem((ROWS, 128), F32),
        vmem((2 * CHUNK, ROWS), BF16),
        vmem((ROWS, 128), F32),
        vmem((2, 8, 128), F32),
        vmem((16, 8, 128), F32),
        vmem((RING, 128), F32),
        vmem((2 * NSUB, CHUNK, SUB), F32),
        vmem((NZ * NSUB, CHUNK, SUB), BF16),
        vmem((NZ * NSUB, CHUNK, SUB), BF16),
        vmem(((NZ - 1) * NSUB, CHUNK, SUB), BF16),
        vmem(((NZ - 1) * NSUB, CHUNK, SUB), BF16),
        dma((11,)),
        dma(()),
        dma(()), dma((11,)), dma(()), dma((11,)),
        dma((2,)), dma((14,)),
        dma(()), dma(()),
        dma(()), dma((NZ * NSUB,)),
        dma(()), dma(((NZ - 1) * NSUB,)),
    ]
    losses, stream_grad, vocab_grad = pl.pallas_call(
        kernel,
        out_shape=(
            pltpu.VMEM((1, BLOCK), F32),
            pltpu.VMEM((BLOCK, WIDTH), F32),
            pltpu.VMEM((CHUNK, COLS), F32),
        ),
        in_specs=[hbm] * 9,
        out_specs=(pl.BlockSpec(memory_space=pltpu.VMEM),) * 3,
        scratch_shapes=scratch,
        compiler_params=pltpu.CompilerParams(
            collective_id=0, has_side_effects=True, vmem_limit_bytes=60 * 1024 * 1024
        ),
    )(hid, down, res, pg.reshape(1, WIDTH), fg.reshape(1, WIDTH), voc,
      bias.reshape(1, COLS), ids.T, wts.T)
    return losses.reshape(BLOCK), stream_grad, vocab_grad


def solution(mesh):
    split = Mesh(mesh.devices.reshape(4, 4, 8, 2), AXES)
    vp, dp = ("y", "x"), ("z", "c")
    return jax.shard_map(
        shards,
        mesh=split,
        in_specs=(
            P(dp, vp),
            P(vp, None),
            P(dp + vp, None),
            P(),
            P(),
            P(None, vp),
            P(vp),
            P(dp, None),
            P(dp, None),
        ),
        out_specs=(P(dp + vp), P(dp + vp, None), P(dp, vp)),
        check_vma=False,
    )
```

```python
import jax
import jax.numpy as jnp
from jax import lax
from jax.experimental import pallas as pl
from jax.experimental.pallas import tpu as pltpu
from jax.sharding import Mesh
from jax.sharding import PartitionSpec as P

MESH = pl.DeviceIdType.MESH
F32 = jnp.float32
BF16 = jnp.bfloat16
AXES = ("y", "x", "z", "c")

EPSILON = 1e-06
Z_WEIGHT = 0.001
LOSS_SCALE = 32.0

RING = 4
NZ = 8
BLOCK = 32
HALF = 16
CHUNK = 128
ROWS = 512
WIDTH = 2048
COLS = 2048
SUB = 512
NSUB = COLS // SUB
RS_ORDER = (2, 1, 3, 0)
AG_ORDER = (0, 3, 1, 2)


def inverse_rms(values):
    return lax.rsqrt(jnp.mean(values * values, axis=-1, keepdims=True) + EPSILON)


def aligned(start, size, unit):
    return pl.ds(pl.multiple_of(start, unit), size)


def kernel(
    hid, down, res, pg, fg, voc, bias, ids, wts,
    loss_o, sg_o, vg_o,
    hid_v, down_v, res_v, pg_v, fg_v, voc_v, bias_v, ids_v, wts_v, meta_v,
    part, scores, wanted, normed, grads, stream_v, inv_v,
    ra, rb, rc, sb2, ra2, rb2, rc2, keep2,
    rra, rrb, rrc, rsb2, rra2, rrb2, rrc2,
    stat_c, turn_v, norm_c, stat_s, stat_r, loss_v,
    v_own, pair_s, pair_r, z_s, z_r,
    load_sem, hid_sem,
    rs_ss, rs_rs, rr_ss, rr_rs, ag_ss, ag_rs, st_ss, st_rs, pr_ss, pr_rs, z_ss, z_rs,
):
    y, x, z, c = (lax.axis_index(name) for name in AXES)
    a = x + c * (y - x)
    b = y + c * (x - y)

    def mod4(value):
        return lax.rem(value, RING)

    def dev(step_a, step_b):
        to_a, to_b = mod4(a + step_a), mod4(b + step_b)
        return (to_b + c * (to_a - to_b), to_a + c * (to_b - to_a), z, c)

    up_z = lax.rem(z + 1 + c * (NZ - 2), NZ)
    down_z = lax.rem(z + NZ - 1 - c * (NZ - 2), NZ)
    dev_up = (y, x, up_z, c)
    dev_down = (y, x, down_z, c)
    dev_pair = (y, x, z, 1 - c)

    def source_row(i, q):
        return (i * (1 + 3 * c) + q * (4 - 3 * c)) * BLOCK

    def rows(i, q, h):
        return aligned(i * CHUNK + q * BLOCK + h * HALF, HALF, HALF)

    def rows32(i, q):
        return aligned(i * CHUNK + q * BLOCK, BLOCK, BLOCK)

    def chunk_rows(i):
        return aligned(i * CHUNK, CHUNK, CHUNK)

    def sub_cols(j):
        return aligned(j * SUB, SUB, SUB)

    def remote(src, dst, send, recv, to):
        return pltpu.make_async_remote_copy(
            src_ref=src, dst_ref=dst, send_sem=send, recv_sem=recv,
            device_id=to, device_id_type=MESH,
        )

    def arrived(view, sem):
        remote(view, view, sem, sem, dev_pair).wait_recv()

    def gone(view, sem):
        remote(view, view, sem, sem, dev_pair).wait_send()

    a_up, a_dn, b_up, b_dn = dev(1, 0), dev(3, 0), dev(0, 1), dev(0, 3)

    barrier = pltpu.get_barrier_semaphore()
    for to in (a_up, a_dn, b_up, b_dn, dev_pair, dev_down):
        pl.semaphore_signal(barrier, inc=1, device_id=to, device_id_type=MESH)

    hid_copies = []
    for i in range(RING):
        for q in range(RING):
            hid_copies.append(
                pltpu.make_async_copy(
                    hid.at[aligned(source_row(i, q), BLOCK, BLOCK), :],
                    hid_v.at[pl.ds(i * CHUNK + q * BLOCK, BLOCK), :],
                    hid_sem,
                )
            )
    pairs = [(down.at[:, pl.ds(k * SUB, SUB)], down_v.at[:, pl.ds(k * SUB, SUB)]) for k in range(4)]
    pairs += [
        (ids, ids_v), (wts, wts_v), (res, res_v), (pg, pg_v), (fg, fg_v), (bias, bias_v),
    ]
    pairs += [
        (voc.at[pl.ds(k * SUB, SUB), :], voc_v.at[pl.ds(k * SUB, SUB), :]) for k in range(4)
    ]
    loads = [
        pltpu.make_async_copy(src, dst, load_sem.at[min(k, 10)])
        for k, (src, dst) in enumerate(pairs)
    ]
    for copy in hid_copies + loads[0:4]:
        copy.start()

    def branch_chunk(i, send, ready=None):
        def piece(n, carry):
            value = jnp.dot(
                hid_v[chunk_rows(i), :], down_v[:, sub_cols(n)], preferred_element_type=F32
            )
            if ready is None:
                scores[chunk_rows(i), sub_cols(n)] = value
            if send:
                part[chunk_rows(i), sub_cols(n)] = value.astype(BF16)
            return carry

        if ready is None:
            lax.fori_loop(0, WIDTH // SUB, piece, 0)
        else:
            for n in range(WIDTH // SUB):
                ready[n].wait()
                piece(n, 0)

    def rs_tools(ra, rb, rc, sb2, ra2, rb2, rc2, ss, rs):
        far, up, dn = mod4(a + 2), mod4(a + 1), mod4(a + 3)

        def q_of(t):
            return mod4(b + RS_ORDER[t])

        def one(kind, t):
            q = q_of(t)
            src, dst, to = (
                (rows(far, q, 0), ra.at[0, t], a_up),
                (rows(far, q, 1), ra.at[1, t], a_dn),
                (rows(up, q, 1), rb.at[0, t], a_up),
                (rows(dn, q, 0), rb.at[1, t], a_dn),
                (rows(up, q, 0), rc.at[0, t], a_up),
                (rows(dn, q, 1), rc.at[1, t], a_dn),
            )[kind]
            recv = rs.at[t if kind < 2 else RING + t]
            return remote(part.at[src, :], dst, ss, recv, to)

        def two(kind):
            src, dst, to = (
                (sb2.at[0, 0], ra2.at[0], b_up),
                (sb2.at[0, 1], ra2.at[1], b_dn),
                (sb2.at[1, 1], rb2.at[0], b_up),
                (sb2.at[2, 0], rb2.at[1], b_dn),
                (sb2.at[1, 0], rc2.at[0], b_up),
                (sb2.at[2, 1], rc2.at[1], b_dn),
            )[kind]
            return remote(src, dst, ss, rs.at[8 + min(kind, 2)], to)

        def first(turns):
            for t in turns:
                one(0, t).start()
                one(1, t).start()

        def second(turns):
            for t in turns:
                one(2, t).start()
                one(3, t).start()

        def third(turns):
            for t in turns:
                q = q_of(t)
                arrived(ra.at[:, t], rs.at[t])
                for kind, i, h in ((0, up, 0), (1, dn, 1)):
                    part[rows(i, q, h), :] = (
                        scores[rows(i, q, h), :] + ra[h, t].astype(F32)
                    ).astype(BF16)
                    one(4 + kind, t).start()

        def finish_a(turns):
            for t in turns:
                q = q_of(t)
                arrived(part.at[pl.ds(0, 4 * HALF), :], rs.at[RING + t])
                low = scores[rows(a, q, 0), :] + rc[0, t].astype(F32) + rb[1, t].astype(F32)
                high = scores[rows(a, q, 1), :] + rb[0, t].astype(F32) + rc[1, t].astype(F32)
                if t == 0:
                    sb2[0, 0] = low.astype(BF16)
                    two(0).start()
                    sb2[0, 1] = high.astype(BF16)
                    two(1).start()
                elif t == 1:
                    sb2[1, 1] = high.astype(BF16)
                    two(2).start()
                    keep2[0] = low
                elif t == 2:
                    sb2[2, 0] = low.astype(BF16)
                    two(3).start()
                    keep2[1] = high
                else:
                    keep2[2] = low
                    keep2[3] = high

        def middle_b():
            two(0).wait_recv()
            sb2[1, 0] = (keep2[0] + ra2[0].astype(F32)).astype(BF16)
            two(4).start()
            two(1).wait_recv()
            sb2[2, 1] = (keep2[1] + ra2[1].astype(F32)).astype(BF16)
            two(5).start()

        def finish_b():
            arrived(part.at[pl.ds(0, 4 * HALF), :], rs.at[10])
            low = keep2[2] + rc2[0].astype(F32) + rb2[1].astype(F32)
            high = keep2[3] + rb2[0].astype(F32) + rc2[1].astype(F32)
            return jnp.concatenate([low, high], axis=0)

        def sent():
            gone(part.at[pl.ds(0, 30 * HALF), :], ss)

        return first, second, third, finish_a, middle_b, finish_b, sent

    def wanted_block(p):
        i, q = p // RING, lax.rem(p, RING)
        at = aligned(source_row(i, q), BLOCK, BLOCK)
        local = meta_v[at, 0:4] - ((y * RING + x) * COLS).astype(F32)
        weight = meta_v[at, 4:8]
        for n in range(NSUB):
            position = (lax.broadcasted_iota(jnp.int32, (BLOCK, SUB), 1) + n * SUB).astype(F32)
            total = jnp.zeros((BLOCK, SUB), F32)
            for k in range(4):
                total = total + jnp.where(
                    local[:, k : k + 1] == position, weight[:, k : k + 1], 0.0
                )
            wanted[aligned(p * BLOCK, BLOCK, BLOCK), pl.ds(n * SUB, SUB)] = total

    def wanted_blocks(start, stop):
        def body(p, carry):
            wanted_block(p)
            return carry

        lax.fori_loop(start, stop, body, 0)

    first, second, third, finish_a, middle_b, finish_b, sent = rs_tools(
        ra, rb, rc, sb2, ra2, rb2, rc2, rs_ss, rs_rs
    )
    pltpu.make_async_copy(hid, hid_v, hid_sem).wait()
    branch_chunk(mod4(a + 2), True, loads[0:4])
    for copy in loads[4:]:
        copy.start()
    pl.semaphore_wait(barrier, 6)
    first((0, 1, 2))
    branch_chunk(mod4(a + 1), True)
    branch_chunk(mod4(a + 3), True)
    second((0, 1))
    branch_chunk(a, False)
    third((0, 1))
    second((2,))
    third((2,))
    first((3,))
    second((3,))
    for copy in loads[4:10]:
        copy.wait()
    for g in range(RING):
        lanes = pl.ds(g * 128, 128)
        both = jnp.concatenate([ids_v[:, lanes].astype(F32), wts_v[:, lanes]], axis=0)
        meta_v[lanes, :] = jnp.transpose(jnp.concatenate([both] * 16, axis=0))
    wanted_blocks(0, 8)
    finish_a((0,))
    wanted_blocks(8, 16)
    finish_a((1, 2))
    middle_b()
    third((3,))
    finish_a((3,))
    branch = finish_b()

    stream = res_v[...].astype(F32) + branch * inverse_rms(branch) * pg_v[...]
    inverse = inverse_rms(stream)
    stream_v[...] = stream
    inv_v[...] = jnp.broadcast_to(inverse, inv_v.shape)
    normed[rows32(a, b), :] = (stream * inverse * fg_v[...]).astype(BF16)

    up, dn, far = mod4(a + 1), mod4(a + 3), mod4(a + 2)
    b1, b3, b2 = mod4(b + 1), mod4(b + 3), mod4(b + 2)

    def gather_b(kind):
        at, to = (
            (rows(a, b, 0), b_up),
            (rows(a, b, 1), b_dn),
            (rows(a, b, 1), b_up),
            (rows(a, b, 0), b_dn),
            (rows(a, b3, 0), b_up),
            (rows(a, b1, 1), b_dn),
        )[kind]
        recv = ag_rs.at[(0, 1, 2, 2, 3, 3)[kind]]
        return remote(normed.at[at, :], normed.at[at, :], ag_ss, recv, to)

    def gather_a(kind, t):
        q = mod4(b + AG_ORDER[t])
        at, to = (
            (rows32(a, q), a_up),
            (rows32(a, q), a_dn),
            (rows(dn, q, 0), a_up),
            (rows(up, q, 1), a_dn),
            (rows(a, q, 0), a_up),
            (rows(a, q, 1), a_dn),
            (rows(a, q, 1), a_up),
            (rows(a, q, 0), a_dn),
        )[kind]
        recv = ag_rs.at[(4 + 2 * t, 5 + 2 * t, 12, 12, 10, 11, 13, 13)[kind]]
        return remote(normed.at[at, :], normed.at[at, :], ag_ss, recv, to)

    def forward_a(t):
        q = mod4(b + AG_ORDER[t])
        for kind, i in ((0, dn), (1, up)):
            at = rows32(i, q) if t < 3 else rows(i, q, kind)
            arrived(normed.at[at, :], ag_rs.at[4 + 2 * t + kind])
            gather_a(2 + kind, t).start()

    for kind in range(4):
        gather_b(kind).start()

    for kind in (0, 1):
        gather_a(kind, 0).start()
    for kind, q in ((0, b3), (1, b1)):
        arrived(normed.at[rows(a, q, kind), :], ag_rs.at[kind])
        gather_b(4 + kind).start()
    arrived(normed.at[pl.ds(0, BLOCK), :], ag_rs.at[2])

    def second_a():
        for t in (1, 2):
            for kind in (0, 1):
                gather_a(kind, t).start()

    @pl.when(c == 0)
    def _():
        second_a()
        forward_a(0)

    arrived(normed.at[rows32(a, b2), :], ag_rs.at[3])
    pl.when(c == 1)(second_a)
    for kind in (4, 5, 6, 7):
        gather_a(kind, 3).start()

    @pl.when(c == 1)
    def _():
        forward_a(0)

    pltpu.make_async_copy(voc, voc_v, load_sem.at[10]).wait()

    def score_pieces(places, start, stop):
        def piece(n, carry):
            rows_in = [normed[at, :] for at in places]
            value = jnp.dot(
                jnp.concatenate(rows_in, axis=0), voc_v[:, sub_cols(n)], preferred_element_type=F32
            ) + bias_v[:, sub_cols(n)]
            first_row = 0
            for at in places:
                scores[at, sub_cols(n)] = value[first_row : first_row + at.size]
                first_row += at.size
            return carry

        lax.fori_loop(start, stop, piece, 0)

    def stats(places):
        groups = [pl.ds(g * 128, 128) for g in range(COLS // 128)]
        for at in places:
            peak = scores[at, groups[0]]
            for group in groups[1:]:
                peak = jnp.maximum(peak, scores[at, group])
            peak = jnp.broadcast_to(jnp.max(peak, axis=1, keepdims=True), (at.size, 128))
            total = jnp.zeros((at.size, 128), F32)
            target = jnp.zeros((at.size, 128), F32)
            for group in groups:
                value = scores[at, group]
                total = total + jnp.exp(value - peak)
                target = target + wanted[at, group] * value
            lse = peak + jnp.log(jnp.sum(total, axis=1, keepdims=True))
            first_lane = lax.broadcasted_iota(jnp.int32, (at.size, 128), 1) == 0
            stat_c[at, :] = jnp.where(first_lane, lse, jnp.sum(target, axis=1, keepdims=True))

    def rows64(i):
        return [aligned(i * CHUNK + r * 64, 64, 64) for r in range(2)]

    early = [rows32(i, mod4(b + AG_ORDER[t])) for i in (up, dn) for t in range(3)]
    late = [rows32(up, b2), rows32(dn, b2)]
    score_pieces([chunk_rows(a)], 0, 2)
    forward_a(1)
    score_pieces([chunk_rows(a)], 2, 4)
    forward_a(2)
    score_pieces(early, 0, 2)
    forward_a(3)
    score_pieces(early, 2, 4)
    stats(rows64(a))
    stats(early)
    arrived(normed.at[rows32(a, b), :], ag_rs.at[13])
    arrived(normed.at[chunk_rows(far), :], ag_rs.at[12])
    score_pieces(late + [chunk_rows(far)], 0, 4)
    stats(late + rows64(far))
    for i in range(RING):
        turned = jnp.transpose(stat_c[pl.ds(i * CHUNK, CHUNK), :])
        stat_s[0, i : i + 1, :] = turned[0:1, :]
        stat_s[0, i + RING : i + RING + 1, :] = turned[1:2, :]

    def stat_copy(k):
        return remote(stat_s.at[0], stat_r.at[k], st_ss, st_rs, dev(k // RING, k % RING))

    def vocab_rows(s):
        away = (1 - 2 * c) * (1 + s)
        own_dest = lax.rem(z + 2 * NZ - away, NZ) * 2 + c
        pair_dest = lax.rem(z + 2 * NZ + away, NZ) * 2 + 1 - c
        return jnp.concatenate(
            [normed[:, aligned(dest * CHUNK, CHUNK, CHUNK)] for dest in (own_dest, pair_dest)], axis=1
        )

    is_lse = lax.broadcasted_iota(jnp.int32, (8, 128), 0) < RING
    for k in (10, 9, 11, 6, 14, 5, 7, 13, 15, 2, 8, 1, 3, 4, 12):
        stat_copy(k).start()
    turn_v[...] = jnp.transpose(vocab_rows(0))
    arrived(stat_r.at[pl.ds(1, 15)], st_rs)
    parts = [stat_s[0]] + [stat_r[k] for k in range(1, 16)]
    peak = parts[0]
    for value in parts[1:]:
        peak = jnp.maximum(peak, value)
    joint = peak + jnp.log(sum(jnp.exp(value - peak) for value in parts))
    stat_s[1] = jnp.where(is_lse, joint, sum(parts))
    log_rows = stat_s[1, 0:RING, :]
    for i in range(RING):
        norm_c[pl.ds(i * CHUNK, CHUNK), :] = jnp.transpose(
            jnp.broadcast_to(stat_s[1, i : i + 1, :], (CHUNK, 128))
        )
    loss_v[...] = log_rows - stat_s[1, RING:8, :] + Z_WEIGHT * log_rows * log_rows

    def grad_block(j):
        def body(r, carry):
            at = aligned(r * 64, 64, 64)
            log_norm = norm_c[at, :]
            factor = 1.0 + 2.0 * Z_WEIGHT * log_norm
            for n in range(SUB // 128):
                cols = aligned(j * SUB + n * 128, 128, 128)
                probability = jnp.exp(scores[at, cols] - log_norm)
                grads[at, cols] = (
                    LOSS_SCALE * (probability * factor - wanted[at, cols])
                ).astype(BF16)
            return carry

        lax.fori_loop(0, ROWS // 64, body, 0)

    def pair_copy(s, j):
        k = s * NSUB + j
        return remote(pair_s.at[k], pair_r.at[k], pr_ss, pr_rs.at[k], dev_pair)

    def z_copy(s, j):
        k = s * NSUB + j
        return remote(z_s.at[k], z_r.at[k], z_ss, z_rs.at[k], dev_up)

    def vocab_piece(s, j):
        if s == 0:
            value = jnp.dot(turn_v[...], grads[:, sub_cols(j)], preferred_element_type=F32)
        else:
            value = lax.dot_general(
                vocab_rows(s), grads[:, sub_cols(j)], (((0,), (0,)), ((), ())),
                preferred_element_type=F32,
            )
        v_own[(s % 2) * NSUB + j] = value[0:CHUNK]
        pair_s[s * NSUB + j] = value[CHUNK:].astype(BF16)
        pair_copy(s, j).start()

    def z_piece(s, j):
        k = s * NSUB + j
        pair_copy(s, j).wait_recv()
        value = v_own[(s % 2) * NSUB + j] + pair_r[k].astype(F32)
        if s > 0:
            z_copy(s - 1, j).wait_recv()
            value = value + z_r[k - NSUB].astype(F32)
        if s < NZ - 1:
            z_s[k] = value.astype(BF16)
            z_copy(s, j).start()
        else:
            vg_o[:, sub_cols(j)] = value

    def row_piece(i, n):
        value = lax.dot_general(
            grads[chunk_rows(i), :], voc_v[sub_cols(n), :],
            (((1,), (1,)), ((), ())), preferred_element_type=F32,
        )
        scores[chunk_rows(i), sub_cols(n)] = value
        part[chunk_rows(i), sub_cols(n)] = value.astype(BF16)

    for j in range(NSUB):
        grad_block(j)
        vocab_piece(0, j)
        if j > 0:
            z_piece(0, j - 1)
    z_piece(0, NSUB - 1)
    sent()

    first, second, third, finish_a, middle_b, finish_b, sent_rows = rs_tools(
        rra, rrb, rrc, rsb2, rra2, rrb2, rrc2, rr_ss, rr_rs
    )
    def drain():
        sent_rows()
        gone(normed.at[pl.ds(0, 30 * HALF), :], ag_ss)
        gone(stat_r.at[pl.ds(1, 15)], st_ss)
        gone(pair_s, pr_ss)

    row_order = (far, up, dn, a)
    for s in range(NZ):

        def slot(j, carry):
            if s > 0:
                z_piece(s, j)
            if s < NZ - 1:
                vocab_piece(s + 1, j)
            if s < RING:
                row_piece(row_order[s], j)
            return carry

        lax.fori_loop(0, NSUB, slot, 0)
        if s == 0:
            first(range(RING))
        elif s == 2:
            second((0, 1))
            third((0,))
            second((2,))
            third((1,))
            second((3,))
            third((2, 3))
        elif s == 4:
            finish_a(range(RING))
        elif s == 5:
            middle_b()
        elif s == 6:
            stream = stream_v[...]
            inverse = inv_v[:, 0:1]
            upstream = finish_b() * fg_v[...]
            sg_o[...] = inverse * (
                upstream
                - stream * inverse * inverse * jnp.mean(upstream * stream, axis=-1, keepdims=True)
            )
            own = jnp.broadcast_to(loss_v[pl.ds(a, 1), :], (8, 128))
            own = pltpu.roll(own, lax.rem(128 - b * BLOCK, 128), 1)
            loss_o[...] = own[0:1, 0:BLOCK]
            drain()

    gone(z_s, z_ss)


def shards(hid, down, res, pg, fg, voc, bias, ids, wts):
    hbm = pl.BlockSpec(memory_space=pl.ANY)
    vmem = pltpu.VMEM
    dma = pltpu.SemaphoreType.DMA
    rs_bufs = [
        vmem((2, RING, HALF, WIDTH), BF16),
        vmem((2, RING, HALF, WIDTH), BF16),
        vmem((2, RING, HALF, WIDTH), BF16),
        vmem((3, 2, HALF, WIDTH), BF16),
        vmem((2, HALF, WIDTH), BF16),
        vmem((2, HALF, WIDTH), BF16),
        vmem((2, HALF, WIDTH), BF16),
    ]
    scratch = [
        vmem((ROWS, 512), BF16),
        vmem((512, WIDTH), BF16),
        vmem((BLOCK, WIDTH), BF16),
        vmem((1, WIDTH), F32),
        vmem((1, WIDTH), F32),
        vmem((WIDTH, COLS), BF16),
        vmem((1, COLS), F32),
        vmem((4, ROWS), jnp.int32),
        vmem((4, ROWS), F32),
        vmem((ROWS, 128), F32),
        vmem((ROWS, WIDTH), BF16),
        vmem((ROWS, COLS), F32),
        vmem((ROWS, COLS), F32),
        vmem((ROWS, WIDTH), BF16),
        vmem((ROWS, COLS), BF16),
        vmem((BLOCK, WIDTH), F32),
        vmem((BLOCK, 128), F32),
        *rs_bufs,
        vmem((4, HALF, WIDTH), F32),
        *rs_bufs,
        vmem((ROWS, 128), F32),
        vmem((2 * CHUNK, ROWS), BF16),
        vmem((ROWS, 128), F32),
        vmem((2, 8, 128), F32),
        vmem((16, 8, 128), F32),
        vmem((RING, 128), F32),
        vmem((2 * NSUB, CHUNK, SUB), F32),
        vmem((NZ * NSUB, CHUNK, SUB), BF16),
        vmem((NZ * NSUB, CHUNK, SUB), BF16),
        vmem(((NZ - 1) * NSUB, CHUNK, SUB), BF16),
        vmem(((NZ - 1) * NSUB, CHUNK, SUB), BF16),
        dma((11,)),
        dma(()),
        dma(()), dma((11,)), dma(()), dma((11,)),
        dma(()), dma((14,)),
        dma(()), dma(()),
        dma(()), dma((NZ * NSUB,)),
        dma(()), dma(((NZ - 1) * NSUB,)),
    ]
    losses, stream_grad, vocab_grad = pl.pallas_call(
        kernel,
        out_shape=(
            pltpu.VMEM((1, BLOCK), F32),
            pltpu.VMEM((BLOCK, WIDTH), F32),
            pltpu.VMEM((CHUNK, COLS), F32),
        ),
        in_specs=[hbm] * 9,
        out_specs=(pl.BlockSpec(memory_space=pltpu.VMEM),) * 3,
        scratch_shapes=scratch,
        compiler_params=pltpu.CompilerParams(
            collective_id=0, has_side_effects=True, vmem_limit_bytes=60 * 1024 * 1024
        ),
    )(hid, down, res, pg.reshape(1, WIDTH), fg.reshape(1, WIDTH), voc,
      bias.reshape(1, COLS), ids.T, wts.T)
    return losses.reshape(BLOCK), stream_grad, vocab_grad


def solution(mesh):
    split = Mesh(mesh.devices.reshape(4, 4, 8, 2), AXES)
    vp, dp = ("y", "x"), ("z", "c")
    return jax.shard_map(
        shards,
        mesh=split,
        in_specs=(
            P(dp, vp),
            P(vp, None),
            P(dp + vp, None),
            P(),
            P(),
            P(None, vp),
            P(vp),
            P(dp, None),
            P(dp, None),
        ),
        out_specs=(P(dp + vp), P(dp + vp, None), P(dp, vp)),
        check_vma=False,
    )
```

```python
import jax
import jax.numpy as jnp
from jax import lax
from jax.experimental import pallas as pl
from jax.experimental.pallas import tpu as pltpu
from jax.sharding import Mesh
from jax.sharding import PartitionSpec as P

MESH = pl.DeviceIdType.MESH
F32 = jnp.float32
BF16 = jnp.bfloat16
AXES = ("y", "x", "z", "c")

EPSILON = 1e-06
Z_WEIGHT = 0.001
LOSS_SCALE = 32.0

RING = 4
NZ = 8
BLOCK = 32
HALF = 16
CHUNK = 128
ROWS = 512
WIDTH = 2048
COLS = 2048
SUB = 512
NSUB = COLS // SUB
RS_ORDER = (2, 1, 3, 0)
AG_ORDER = (0, 3, 1, 2)


def inverse_rms(values):
    return lax.rsqrt(jnp.mean(values * values, axis=-1, keepdims=True) + EPSILON)


def aligned(start, size, unit):
    return pl.ds(pl.multiple_of(start, unit), size)


def kernel(
    hid, down, res, pg, fg, voc, bias, ids, wts,
    loss_o, sg_o, vg_o,
    hid_v, down_v, res_v, pg_v, fg_v, voc_v, bias_v, ids_v, wts_v, meta_v,
    part, scores, wanted, normed, grads, stream_v, inv_v,
    ra, rb, rc, sb2, ra2, rb2, rc2, keep2,
    rra, rrb, rrc, rsb2, rra2, rrb2, rrc2,
    stat_c, turn_v, norm_c, stat_s, stat_r, loss_v,
    v_own, pair_s, pair_r, z_s, z_r,
    load_sem, hid_sem,
    rs_ss, rs_rs, rr_ss, rr_rs, ag_ss, ag_rs, st_ss, st_rs, pr_ss, pr_rs, z_ss, z_rs,
):
    y, x, z, c = (lax.axis_index(name) for name in AXES)
    a = x + c * (y - x)
    b = y + c * (x - y)

    def mod4(value):
        return lax.rem(value, RING)

    def dev(step_a, step_b):
        to_a, to_b = mod4(a + step_a), mod4(b + step_b)
        return (to_b + c * (to_a - to_b), to_a + c * (to_b - to_a), z, c)

    up_z = lax.rem(z + 1 + c * (NZ - 2), NZ)
    down_z = lax.rem(z + NZ - 1 - c * (NZ - 2), NZ)
    dev_up = (y, x, up_z, c)
    dev_down = (y, x, down_z, c)
    dev_pair = (y, x, z, 1 - c)

    def source_row(i, q):
        return (i * (1 + 3 * c) + q * (4 - 3 * c)) * BLOCK

    def rows(i, q, h):
        return aligned(i * CHUNK + q * BLOCK + h * HALF, HALF, HALF)

    def rows32(i, q):
        return aligned(i * CHUNK + q * BLOCK, BLOCK, BLOCK)

    def chunk_rows(i):
        return aligned(i * CHUNK, CHUNK, CHUNK)

    def sub_cols(j):
        return aligned(j * SUB, SUB, SUB)

    def wide_cols(j):
        return aligned(j * 2 * SUB, 2 * SUB, 2 * SUB)

    def remote(src, dst, send, recv, to):
        return pltpu.make_async_remote_copy(
            src_ref=src, dst_ref=dst, send_sem=send, recv_sem=recv,
            device_id=to, device_id_type=MESH,
        )

    def arrived(view, sem):
        remote(view, view, sem, sem, dev_pair).wait_recv()

    def gone(view, sem):
        remote(view, view, sem, sem, dev_pair).wait_send()

    a_up, a_dn, b_up, b_dn = dev(1, 0), dev(3, 0), dev(0, 1), dev(0, 3)

    barrier = pltpu.get_barrier_semaphore()
    for to in (a_up, a_dn, b_up, b_dn, dev_pair, dev_down):
        pl.semaphore_signal(barrier, inc=1, device_id=to, device_id_type=MESH)

    hid_copies = []
    for i in range(RING):
        for q in range(RING):
            hid_copies.append(
                pltpu.make_async_copy(
                    hid.at[aligned(source_row(i, q), BLOCK, BLOCK), :],
                    hid_v.at[pl.ds(i * CHUNK + q * BLOCK, BLOCK), :],
                    hid_sem,
                )
            )
    pairs = [(down.at[:, pl.ds(k * SUB, SUB)], down_v.at[:, pl.ds(k * SUB, SUB)]) for k in range(4)]
    pairs += [
        (ids, ids_v), (wts, wts_v), (res, res_v), (pg, pg_v), (fg, fg_v), (bias, bias_v),
    ]
    pairs += [
        (voc.at[pl.ds(k * SUB, SUB), :], voc_v.at[pl.ds(k * SUB, SUB), :]) for k in range(4)
    ]
    loads = [
        pltpu.make_async_copy(src, dst, load_sem.at[min(k, 10)])
        for k, (src, dst) in enumerate(pairs)
    ]
    for copy in hid_copies + loads[0:4]:
        copy.start()

    def branch_chunk(i, send, ready=None):
        def piece(n, carry):
            value = jnp.dot(
                hid_v[chunk_rows(i), :], down_v[:, sub_cols(n)], preferred_element_type=F32
            )
            if ready is None:
                scores[chunk_rows(i), sub_cols(n)] = value
            if send:
                part[chunk_rows(i), sub_cols(n)] = value.astype(BF16)
            return carry

        if ready is None:
            lax.fori_loop(0, WIDTH // SUB, piece, 0)
        else:
            for n in range(WIDTH // SUB):
                ready[n].wait()
                piece(n, 0)

    def rs_tools(ra, rb, rc, sb2, ra2, rb2, rc2, ss, rs):
        far, up, dn = mod4(a + 2), mod4(a + 1), mod4(a + 3)

        def q_of(t):
            return mod4(b + RS_ORDER[t])

        def one(kind, t):
            q = q_of(t)
            src, dst, to = (
                (rows(far, q, 0), ra.at[0, t], a_up),
                (rows(far, q, 1), ra.at[1, t], a_dn),
                (rows(up, q, 1), rb.at[0, t], a_up),
                (rows(dn, q, 0), rb.at[1, t], a_dn),
                (rows(up, q, 0), rc.at[0, t], a_up),
                (rows(dn, q, 1), rc.at[1, t], a_dn),
            )[kind]
            recv = rs.at[t if kind < 2 else RING + t]
            return remote(part.at[src, :], dst, ss, recv, to)

        def two(kind):
            src, dst, to = (
                (sb2.at[0, 0], ra2.at[0], b_up),
                (sb2.at[0, 1], ra2.at[1], b_dn),
                (sb2.at[1, 1], rb2.at[0], b_up),
                (sb2.at[2, 0], rb2.at[1], b_dn),
                (sb2.at[1, 0], rc2.at[0], b_up),
                (sb2.at[2, 1], rc2.at[1], b_dn),
            )[kind]
            return remote(src, dst, ss, rs.at[8 + min(kind, 2)], to)

        def first(turns):
            for t in turns:
                one(0, t).start()
                one(1, t).start()

        def second(turns):
            for t in turns:
                one(2, t).start()
                one(3, t).start()

        def third(turns):
            for t in turns:
                q = q_of(t)
                arrived(ra.at[:, t], rs.at[t])
                for kind, i, h in ((0, up, 0), (1, dn, 1)):
                    part[rows(i, q, h), :] = (
                        scores[rows(i, q, h), :] + ra[h, t].astype(F32)
                    ).astype(BF16)
                    one(4 + kind, t).start()

        def finish_a(turns):
            for t in turns:
                q = q_of(t)
                arrived(part.at[pl.ds(0, 4 * HALF), :], rs.at[RING + t])
                low = scores[rows(a, q, 0), :] + rc[0, t].astype(F32) + rb[1, t].astype(F32)
                high = scores[rows(a, q, 1), :] + rb[0, t].astype(F32) + rc[1, t].astype(F32)
                if t == 0:
                    sb2[0, 0] = low.astype(BF16)
                    two(0).start()
                    sb2[0, 1] = high.astype(BF16)
                    two(1).start()
                elif t == 1:
                    sb2[1, 1] = high.astype(BF16)
                    two(2).start()
                    keep2[0] = low
                elif t == 2:
                    sb2[2, 0] = low.astype(BF16)
                    two(3).start()
                    keep2[1] = high
                else:
                    keep2[2] = low
                    keep2[3] = high

        def middle_b():
            two(0).wait_recv()
            sb2[1, 0] = (keep2[0] + ra2[0].astype(F32)).astype(BF16)
            two(4).start()
            two(1).wait_recv()
            sb2[2, 1] = (keep2[1] + ra2[1].astype(F32)).astype(BF16)
            two(5).start()

        def finish_b():
            arrived(part.at[pl.ds(0, 4 * HALF), :], rs.at[10])
            low = keep2[2] + rc2[0].astype(F32) + rb2[1].astype(F32)
            high = keep2[3] + rb2[0].astype(F32) + rc2[1].astype(F32)
            return jnp.concatenate([low, high], axis=0)

        def sent():
            gone(part.at[pl.ds(0, 30 * HALF), :], ss)

        return first, second, third, finish_a, middle_b, finish_b, sent

    def wanted_block(p):
        i, q = p // RING, lax.rem(p, RING)
        at = aligned(source_row(i, q), BLOCK, BLOCK)
        local = meta_v[at, 0:4] - ((y * RING + x) * COLS).astype(F32)
        weight = meta_v[at, 4:8]
        for n in range(NSUB):
            position = (lax.broadcasted_iota(jnp.int32, (BLOCK, SUB), 1) + n * SUB).astype(F32)
            total = jnp.zeros((BLOCK, SUB), F32)
            for k in range(4):
                total = total + jnp.where(
                    local[:, k : k + 1] == position, weight[:, k : k + 1], 0.0
                )
            wanted[aligned(p * BLOCK, BLOCK, BLOCK), pl.ds(n * SUB, SUB)] = total

    def wanted_blocks(start, stop):
        def body(p, carry):
            wanted_block(p)
            return carry

        lax.fori_loop(start, stop, body, 0)

    first, second, third, finish_a, middle_b, finish_b, sent = rs_tools(
        ra, rb, rc, sb2, ra2, rb2, rc2, rs_ss, rs_rs
    )
    pltpu.make_async_copy(hid, hid_v, hid_sem).wait()
    branch_chunk(mod4(a + 2), True, loads[0:4])
    for copy in loads[4:]:
        copy.start()
    pl.semaphore_wait(barrier, 6)
    first((0, 1, 2))
    branch_chunk(mod4(a + 1), True)
    branch_chunk(mod4(a + 3), True)
    second((0, 1))
    branch_chunk(a, False)
    third((0, 1))
    second((2,))
    third((2,))
    first((3,))
    second((3,))
    for copy in loads[4:10]:
        copy.wait()
    for g in range(RING):
        lanes = pl.ds(g * 128, 128)
        both = jnp.concatenate([ids_v[:, lanes].astype(F32), wts_v[:, lanes]], axis=0)
        meta_v[lanes, :] = jnp.transpose(jnp.concatenate([both] * 16, axis=0))
    wanted_blocks(0, 8)
    finish_a((0,))
    wanted_blocks(8, 16)
    finish_a((1,))
    third((3,))
    finish_a((2,))
    middle_b()
    finish_a((3,))
    branch = finish_b()

    stream = res_v[...].astype(F32) + branch * inverse_rms(branch) * pg_v[...]
    inverse = inverse_rms(stream)
    stream_v[...] = stream
    inv_v[...] = jnp.broadcast_to(inverse, inv_v.shape)
    normed[rows32(a, b), :] = (stream * inverse * fg_v[...]).astype(BF16)

    up, dn, far = mod4(a + 1), mod4(a + 3), mod4(a + 2)
    b1, b3, b2 = mod4(b + 1), mod4(b + 3), mod4(b + 2)

    def gather_b(kind):
        at, to = (
            (rows(a, b, 0), b_up),
            (rows(a, b, 1), b_dn),
            (rows(a, b, 1), b_up),
            (rows(a, b, 0), b_dn),
            (rows(a, b3, 0), b_up),
            (rows(a, b1, 1), b_dn),
        )[kind]
        recv = ag_rs.at[(0, 1, 2, 2, 3, 3)[kind]]
        return remote(normed.at[at, :], normed.at[at, :], ag_ss, recv, to)

    def gather_a(kind, t):
        q = mod4(b + AG_ORDER[t])
        at, to = (
            (rows32(a, q), a_up),
            (rows32(a, q), a_dn),
            (rows(dn, q, 0), a_up),
            (rows(up, q, 1), a_dn),
            (rows(a, q, 0), a_up),
            (rows(a, q, 1), a_dn),
            (rows(a, q, 1), a_up),
            (rows(a, q, 0), a_dn),
        )[kind]
        recv = ag_rs.at[(4 + 2 * t, 5 + 2 * t, 12, 12, 10, 11, 13, 13)[kind]]
        return remote(normed.at[at, :], normed.at[at, :], ag_ss, recv, to)

    def forward_a(t):
        q = mod4(b + AG_ORDER[t])
        for kind, i in ((0, dn), (1, up)):
            at = rows32(i, q) if t < 3 else rows(i, q, kind)
            arrived(normed.at[at, :], ag_rs.at[4 + 2 * t + kind])
            gather_a(2 + kind, t).start()

    for kind in range(4):
        gather_b(kind).start()

    for kind in (0, 1):
        gather_a(kind, 0).start()
    for kind, q in ((0, b3), (1, b1)):
        arrived(normed.at[rows(a, q, kind), :], ag_rs.at[kind])
        gather_b(4 + kind).start()
    arrived(normed.at[pl.ds(0, BLOCK), :], ag_rs.at[2])

    def second_a():
        for t in (1, 2):
            for kind in (0, 1):
                gather_a(kind, t).start()

    @pl.when(c == 0)
    def _():
        second_a()
        forward_a(0)

    arrived(normed.at[rows32(a, b2), :], ag_rs.at[3])
    pl.when(c == 1)(second_a)
    for kind in (4, 5, 6, 7):
        gather_a(kind, 3).start()

    @pl.when(c == 1)
    def _():
        forward_a(0)

    pltpu.make_async_copy(voc, voc_v, load_sem.at[10]).wait()

    def score_pieces(places, start, stop):
        def piece(n, carry):
            rows_in = [normed[at, :] for at in places]
            value = jnp.dot(
                jnp.concatenate(rows_in, axis=0), voc_v[:, wide_cols(n)], preferred_element_type=F32
            ) + bias_v[:, wide_cols(n)]
            first_row = 0
            for at in places:
                scores[at, wide_cols(n)] = value[first_row : first_row + at.size]
                first_row += at.size
            return carry

        lax.fori_loop(start, stop, piece, 0)

    def stats(places):
        groups = [pl.ds(g * 128, 128) for g in range(COLS // 128)]
        for at in places:
            peak = scores[at, groups[0]]
            for group in groups[1:]:
                peak = jnp.maximum(peak, scores[at, group])
            peak = jnp.broadcast_to(jnp.max(peak, axis=1, keepdims=True), (at.size, 128))
            total = jnp.zeros((at.size, 128), F32)
            target = jnp.zeros((at.size, 128), F32)
            for group in groups:
                value = scores[at, group]
                total = total + jnp.exp(value - peak)
                target = target + wanted[at, group] * value
            lse = peak + jnp.log(jnp.sum(total, axis=1, keepdims=True))
            first_lane = lax.broadcasted_iota(jnp.int32, (at.size, 128), 1) == 0
            stat_c[at, :] = jnp.where(first_lane, lse, jnp.sum(target, axis=1, keepdims=True))

    def rows64(i):
        return [aligned(i * CHUNK + r * 64, 64, 64) for r in range(2)]

    early = [rows32(i, mod4(b + AG_ORDER[t])) for i in (up, dn) for t in range(3)]
    late = [rows32(up, b2), rows32(dn, b2)]
    score_pieces([chunk_rows(a)], 0, 1)
    forward_a(1)
    score_pieces([chunk_rows(a)], 1, 2)
    forward_a(2)
    score_pieces(early, 0, 1)
    forward_a(3)
    score_pieces(early, 1, 2)
    stats(rows64(a))
    stats(early)
    arrived(normed.at[rows32(a, b), :], ag_rs.at[13])
    arrived(normed.at[chunk_rows(far), :], ag_rs.at[12])
    score_pieces(late + [chunk_rows(far)], 0, 2)
    stats(late + rows64(far))
    for i in range(RING):
        turned = jnp.transpose(stat_c[pl.ds(i * CHUNK, CHUNK), :])
        stat_s[0, i : i + 1, :] = turned[0:1, :]
        stat_s[0, i + RING : i + RING + 1, :] = turned[1:2, :]

    def stat_copy(k):
        return remote(stat_s.at[0], stat_r.at[k], st_ss, st_rs, dev(k // RING, k % RING))

    def vocab_rows(s):
        away = (1 - 2 * c) * (1 + s)
        own_dest = lax.rem(z + 2 * NZ - away, NZ) * 2 + c
        pair_dest = lax.rem(z + 2 * NZ + away, NZ) * 2 + 1 - c
        return jnp.concatenate(
            [normed[:, aligned(dest * CHUNK, CHUNK, CHUNK)] for dest in (own_dest, pair_dest)], axis=1
        )

    is_lse = lax.broadcasted_iota(jnp.int32, (8, 128), 0) < RING
    for k in (10, 9, 11, 6, 14, 5, 7, 13, 15, 2, 8, 1, 3, 4, 12):
        stat_copy(k).start()
    turn_v[...] = jnp.transpose(vocab_rows(0))
    arrived(stat_r.at[pl.ds(1, 15)], st_rs)
    parts = [stat_s[0]] + [stat_r[k] for k in range(1, 16)]
    peak = parts[0]
    for value in parts[1:]:
        peak = jnp.maximum(peak, value)
    joint = peak + jnp.log(sum(jnp.exp(value - peak) for value in parts))
    stat_s[1] = jnp.where(is_lse, joint, sum(parts))
    log_rows = stat_s[1, 0:RING, :]
    for i in range(RING):
        norm_c[pl.ds(i * CHUNK, CHUNK), :] = jnp.transpose(
            jnp.broadcast_to(stat_s[1, i : i + 1, :], (CHUNK, 128))
        )
    loss_v[...] = log_rows - stat_s[1, RING:8, :] + Z_WEIGHT * log_rows * log_rows

    def grad_block(j):
        def body(r, carry):
            at = aligned(r * 64, 64, 64)
            log_norm = norm_c[at, :]
            factor = 1.0 + 2.0 * Z_WEIGHT * log_norm
            for n in range(SUB // 128):
                cols = aligned(j * SUB + n * 128, 128, 128)
                probability = jnp.exp(scores[at, cols] - log_norm)
                grads[at, cols] = (
                    LOSS_SCALE * (probability * factor - wanted[at, cols])
                ).astype(BF16)
            return carry

        lax.fori_loop(0, ROWS // 64, body, 0)

    def pair_copy(s, j):
        k = s * NSUB + j
        return remote(pair_s.at[k], pair_r.at[k], pr_ss, pr_rs.at[k], dev_pair)

    def z_copy(s, j):
        k = s * NSUB + j
        return remote(z_s.at[k], z_r.at[k], z_ss, z_rs.at[k], dev_up)

    def vocab_piece(s, j):
        if s == 0:
            value = jnp.dot(turn_v[...], grads[:, sub_cols(j)], preferred_element_type=F32)
        else:
            value = lax.dot_general(
                vocab_rows(s), grads[:, sub_cols(j)], (((0,), (0,)), ((), ())),
                preferred_element_type=F32,
            )
        v_own[(s % 2) * NSUB + j] = value[0:CHUNK]
        pair_s[s * NSUB + j] = value[CHUNK:].astype(BF16)
        pair_copy(s, j).start()

    def z_piece(s, j):
        k = s * NSUB + j
        pair_copy(s, j).wait_recv()
        value = v_own[(s % 2) * NSUB + j] + pair_r[k].astype(F32)
        if s > 0:
            z_copy(s - 1, j).wait_recv()
            value = value + z_r[k - NSUB].astype(F32)
        if s < NZ - 1:
            z_s[k] = value.astype(BF16)
            z_copy(s, j).start()
        else:
            vg_o[:, sub_cols(j)] = value

    def row_piece(i, n):
        value = lax.dot_general(
            grads[chunk_rows(i), :], voc_v[sub_cols(n), :],
            (((1,), (1,)), ((), ())), preferred_element_type=F32,
        )
        scores[chunk_rows(i), sub_cols(n)] = value
        part[chunk_rows(i), sub_cols(n)] = value.astype(BF16)

    for j in range(NSUB):
        grad_block(j)
        vocab_piece(0, j)
        if j > 0:
            z_piece(0, j - 1)
    z_piece(0, NSUB - 1)
    sent()

    first, second, third, finish_a, middle_b, finish_b, sent_rows = rs_tools(
        rra, rrb, rrc, rsb2, rra2, rrb2, rrc2, rr_ss, rr_rs
    )
    def drain():
        sent_rows()
        gone(normed.at[pl.ds(0, 30 * HALF), :], ag_ss)
        gone(stat_r.at[pl.ds(1, 15)], st_ss)
        gone(pair_s, pr_ss)

    row_order = (far, up, dn, a)
    for s in range(NZ):

        def slot(j, carry):
            if s > 0:
                z_piece(s, j)
            if s < NZ - 1:
                vocab_piece(s + 1, j)
            if s < RING:
                row_piece(row_order[s], j)
            return carry

        lax.fori_loop(0, NSUB, slot, 0)
        if s == 0:
            first(range(RING))
        elif s == 2:
            second((0, 1))
            third((0,))
            second((2,))
            third((1,))
            second((3,))
            third((2, 3))
        elif s == 4:
            finish_a(range(RING))
        elif s == 5:
            middle_b()
        elif s == 6:
            stream = stream_v[...]
            inverse = inv_v[:, 0:1]
            upstream = finish_b() * fg_v[...]
            sg_o[...] = inverse * (
                upstream
                - stream * inverse * inverse * jnp.mean(upstream * stream, axis=-1, keepdims=True)
            )
            own = jnp.broadcast_to(loss_v[pl.ds(a, 1), :], (8, 128))
            own = pltpu.roll(own, lax.rem(128 - b * BLOCK, 128), 1)
            loss_o[...] = own[0:1, 0:BLOCK]
            drain()

    gone(z_s, z_ss)


def shards(hid, down, res, pg, fg, voc, bias, ids, wts):
    hbm = pl.BlockSpec(memory_space=pl.ANY)
    vmem = pltpu.VMEM
    dma = pltpu.SemaphoreType.DMA
    rs_bufs = [
        vmem((2, RING, HALF, WIDTH), BF16),
        vmem((2, RING, HALF, WIDTH), BF16),
        vmem((2, RING, HALF, WIDTH), BF16),
        vmem((3, 2, HALF, WIDTH), BF16),
        vmem((2, HALF, WIDTH), BF16),
        vmem((2, HALF, WIDTH), BF16),
        vmem((2, HALF, WIDTH), BF16),
    ]
    scratch = [
        vmem((ROWS, 512), BF16),
        vmem((512, WIDTH), BF16),
        vmem((BLOCK, WIDTH), BF16),
        vmem((1, WIDTH), F32),
        vmem((1, WIDTH), F32),
        vmem((WIDTH, COLS), BF16),
        vmem((1, COLS), F32),
        vmem((4, ROWS), jnp.int32),
        vmem((4, ROWS), F32),
        vmem((ROWS, 128), F32),
        vmem((ROWS, WIDTH), BF16),
        vmem((ROWS, COLS), F32),
        vmem((ROWS, COLS), F32),
        vmem((ROWS, WIDTH), BF16),
        vmem((ROWS, COLS), BF16),
        vmem((BLOCK, WIDTH), F32),
        vmem((BLOCK, 128), F32),
        *rs_bufs,
        vmem((4, HALF, WIDTH), F32),
        *rs_bufs,
        vmem((ROWS, 128), F32),
        vmem((2 * CHUNK, ROWS), BF16),
        vmem((ROWS, 128), F32),
        vmem((2, 8, 128), F32),
        vmem((16, 8, 128), F32),
        vmem((RING, 128), F32),
        vmem((2 * NSUB, CHUNK, SUB), F32),
        vmem((NZ * NSUB, CHUNK, SUB), BF16),
        vmem((NZ * NSUB, CHUNK, SUB), BF16),
        vmem(((NZ - 1) * NSUB, CHUNK, SUB), BF16),
        vmem(((NZ - 1) * NSUB, CHUNK, SUB), BF16),
        dma((11,)),
        dma(()),
        dma(()), dma((11,)), dma(()), dma((11,)),
        dma(()), dma((14,)),
        dma(()), dma(()),
        dma(()), dma((NZ * NSUB,)),
        dma(()), dma(((NZ - 1) * NSUB,)),
    ]
    losses, stream_grad, vocab_grad = pl.pallas_call(
        kernel,
        out_shape=(
            pltpu.VMEM((1, BLOCK), F32),
            pltpu.VMEM((BLOCK, WIDTH), F32),
            pltpu.VMEM((CHUNK, COLS), F32),
        ),
        in_specs=[hbm] * 9,
        out_specs=(pl.BlockSpec(memory_space=pltpu.VMEM),) * 3,
        scratch_shapes=scratch,
        compiler_params=pltpu.CompilerParams(
            collective_id=0, has_side_effects=True, vmem_limit_bytes=60 * 1024 * 1024
        ),
    )(hid, down, res, pg.reshape(1, WIDTH), fg.reshape(1, WIDTH), voc,
      bias.reshape(1, COLS), ids.T, wts.T)
    return losses.reshape(BLOCK), stream_grad, vocab_grad


def solution(mesh):
    split = Mesh(mesh.devices.reshape(4, 4, 8, 2), AXES)
    vp, dp = ("y", "x"), ("z", "c")
    return jax.shard_map(
        shards,
        mesh=split,
        in_specs=(
            P(dp, vp),
            P(vp, None),
            P(dp + vp, None),
            P(),
            P(),
            P(None, vp),
            P(vp),
            P(dp, None),
            P(dp, None),
        ),
        out_specs=(P(dp + vp), P(dp + vp, None), P(dp, vp)),
        check_vma=False,
    )
```
